32 devices in a mesh: fs: 4 (over y, x), tp: 8 (over z, core).
Axes of the slice: x: 2, y: 2, z: 4, core: 2. Of those that a mesh axis runs over, the one named last changes fastest.
Arguments:
- saved_inputs: bfloat16 [2688, 4096], P('fs', 'tp'), may hold values from -6 to 6
- proj_cotangent: bfloat16 [2688, 4096], P('fs', 'tp'), may hold values from -0.115722656 to 0.115722656
- saved_hidden: bfloat16 [2688, 4096], P('fs', 'tp'), may hold values from -6 to 6
- out_cotangent: bfloat16 [2688, 4096], P('fs', 'tp'), may hold values from -0.115722656 to 0.115722656
- factors: bfloat16 [2, 4096, 128], replicated, may hold values from -0.46875 to 0.46875
- w_proj: float32 [4096, 4096], P('fs', 'tp'), may hold values from -0.09375 to 0.09375
- w_out: float32 [4096, 4096], P('tp', 'fs'), may hold values from -0.09375 to 0.09375
- moment_first: float32 [2, 128, 4096], P(None, None, 'tp'), may hold values from -1.8 to 1.8
- moment_second: float32 [2, 128, 4096], P(None, None, 'tp'), may hold values from 0.05 to 1
Outputs:
- proj_next: float32 [4096, 4096], P('fs', 'tp')
- out_next: float32 [4096, 4096], P('tp', 'fs')
- proj_copy: bfloat16 [4096, 4096], P(None, 'tp')
- out_copy: bfloat16 [4096, 4096], P('tp')
- first_next: float32 [2, 128, 4096], P(None, None, 'tp')
- second_next: float32 [2, 128, 4096], P(None, None, 'tp')
The draws below stay inside these ranges and needn't reach their ends.
All inputs are finite; a program needn't handle non-finite values.
Results may differ from the reference program's by a relative error of at most 0.001.
Values may be sent and summed in bfloat16 or wider, within the bound.
A program may use at most 64 MiB of HBM per device.

```python
import math
import jax
import jax.numpy as jnp
from jax import lax

D = 4096
E = 4096
RANK = 128
TOKENS = 2688


def draw_factors(key, part):
    base_key, rough_key = jax.random.split(jax.random.fold_in(key, 11))
    position = jnp.arange(D, dtype=jnp.float32) / max(D - 1, 1)
    rough = jnp.exp(jax.random.uniform(rough_key, (2, D, 1), jnp.float32, 0.0, math.log(4.0)))
    base = jnp.clip(jax.random.normal(base_key, (2, D, RANK), jnp.float32), -4.0, 4.0)
    rising = jnp.exp(position * math.log(3.0))
    values = base * rough * rising[None, :, None] * (0.5 / math.sqrt(D))
    return values.astype(jnp.bfloat16)


def block_levels(key, dims, pieces, smallest, high):
    def one(axis_at, parts):
        draws = jax.random.uniform(jax.random.fold_in(jax.random.fold_in(key, 6), axis_at), (parts,), jnp.float32, smallest / len(pieces), high / len(pieces))
        return jnp.repeat(jnp.exp(draws), dims[axis_at] // parts).reshape((-1,) + (1,) * (len(dims) - axis_at - 1))

    factor_of = one(*pieces[0])
    for cut in pieces[1:]:
        factor_of = factor_of * one(*cut)
    return factor_of


def scatter_about(stream_key, dims, width, limit, pieces=(), kind=jnp.bfloat16):
    factor_of = block_levels(stream_key, dims, pieces, -0.22, 0.18) if pieces else 1.0
    entries = jax.random.normal(stream_key, dims, jnp.float32) * width * factor_of
    return jnp.minimum(jnp.maximum(entries, -limit), limit).astype(kind)


def setup_inputs(seed: int = 0) -> dict:
    keys = jax.random.split(jax.random.key(seed), 10)
    saved_inputs = scatter_about(keys[0], (TOKENS, D), 1.0, 6.0, ((0, 4), (1, 8)))
    proj_cotangent = scatter_about(keys[1], (TOKENS, E), (TOKENS ** -0.5), 0.115722656, ((0, 4), (1, 8)))
    saved_hidden = scatter_about(keys[2], (TOKENS, E), 1.0, 6.0, ((0, 4), (1, 8)))
    out_cotangent = scatter_about(keys[3], (TOKENS, D), (TOKENS ** -0.5), 0.115722656, ((0, 4), (1, 8)))
    factors = draw_factors(jax.random.fold_in(keys[9], 71), 0)
    w_proj = scatter_about(keys[5], (D, E), D ** -0.5, 0.09375, ((0, 4), (1, 8)), jnp.float32)
    w_out = scatter_about(keys[6], (E, D), E ** -0.5, 0.09375, ((0, 8), (1, 4)), jnp.float32)
    moment_first = scatter_about(keys[7], (2, RANK, E), 0.3, 1.8, ((2, 8),), jnp.float32)
    moment_second = jnp.clip(jnp.exp(math.log(1.0) - 2.9957323 * jax.random.uniform(keys[8], (2, RANK, E), jnp.float32) ** block_levels(keys[8], (2, RANK, E), ((2, 8),), -0.2, 0.2)), 0.05, 1.0)
    return {"saved_inputs": saved_inputs, "proj_cotangent": proj_cotangent, "saved_hidden": saved_hidden, "out_cotangent": out_cotangent, "factors": factors, "w_proj": w_proj, "w_out": w_out, "moment_first": moment_first, "moment_second": moment_second}


beta_first = 0.9
beta_second = 0.95
learn_rate = 0.02
epsilon = 1e-06

def reference(saved_inputs, proj_cotangent, saved_hidden, out_cotangent, factors, w_proj, w_out, moment_first, moment_second):
    highest = lax.Precision.HIGHEST
    factor_full = factors.astype(jnp.float32)
    grad_proj = jnp.dot(saved_inputs.T, proj_cotangent, preferred_element_type=jnp.float32)
    grad_out_t = jnp.dot(out_cotangent.T, saved_hidden, preferred_element_type=jnp.float32)
    small_grads = jnp.stack([jnp.dot(factor_full[0].T, grad_proj, precision=highest), jnp.dot(factor_full[1].T, grad_out_t, precision=highest)])
    first_next = beta_first * moment_first + (1.0 - beta_first) * small_grads
    second_next = beta_second * moment_second + (1.0 - beta_second) * small_grads * small_grads
    direction = first_next / (jnp.sqrt(second_next) + epsilon)
    update_full = jnp.einsum('kdr,kre->kde', factor_full, direction, precision=highest)
    norm_scale = lax.rsqrt(lax.optimization_barrier(jnp.mean(update_full * update_full, axis=(1, 2))) + epsilon)
    stepped = update_full * norm_scale[:, None, None]
    proj_next = w_proj - learn_rate * stepped[0]
    out_next = w_out - learn_rate * stepped[1].T
    return (proj_next, out_next, proj_next.astype(jnp.bfloat16), out_next.astype(jnp.bfloat16), first_next, second_next)
```

```python
import functools

import jax
import jax.numpy as jnp
from jax import lax
from jax.experimental import pallas as pl
from jax.experimental.pallas import tpu as pltpu
from jax.sharding import PartitionSpec as P

beta_first = 0.9
beta_second = 0.95
learn_rate = 0.02
epsilon = 1e-06
weight_gain = 2500.0
code_top = 200.0
chunks = 4
pieces = 16
pad_rows = 16
MIB = 1024 * 1024
MESH = pl.DeviceIdType.MESH


def encode(x, gain, doublings):
    t = x * gain
    for _ in range(doublings):
        t = t * t
    return jnp.where(x < 0, -t, t).astype(jnp.bfloat16)


def decode(code, gain, doublings):
    v = code.astype(jnp.float32)
    size = jnp.exp2(jnp.log2(jnp.abs(v)) * (0.5**doublings)) * (1.0 / gain)
    return jnp.where(v < 0, -size, size)


def largest(x):
    top = jnp.max(jnp.max(jnp.abs(x), axis=0, keepdims=True), axis=1, keepdims=True)
    return jnp.maximum(top, 1e-30)


def two_parts(x, axis):
    high = x.astype(jnp.bfloat16)
    low = (x - high.astype(jnp.float32)).astype(jnp.bfloat16)
    return jnp.concatenate([high, low], axis=axis)


def proj_step(f, d0):
    return jnp.dot(jnp.concatenate([f, f], axis=1), d0[...], preferred_element_type=jnp.float32)


def out_step(f, d1):
    return lax.dot_general(
        d1[...],
        jnp.concatenate([f, f], axis=1),
        (((1,), (1,)), ((), ())),
        preferred_element_type=jnp.float32,
    )


def pack(ref, x):
    top = largest(x).astype(jnp.bfloat16)
    ref[: x.shape[0], :] = encode(x, code_top / top.astype(jnp.float32), 4)
    ref[ref.shape[0] - pad_rows :, :] = jnp.broadcast_to(top, (pad_rows, x.shape[1]))


def unpack(ref, n):
    top = ref[ref.shape[0] - pad_rows :, :][0:1, 0:1].astype(jnp.float32)
    return decode(ref[:n, :], code_top / top, 4)


def exchange_kernel(
    tp_count,
    entries,
    si_hbm,
    pc_hbm,
    sh_hbm,
    oc_hbm,
    f_hbm,
    wp_hbm,
    wo_hbm,
    mf_hbm,
    ms_hbm,
    first_ref,
    second_ref,
    d0_ref,
    d1_ref,
    gp_ref,
    go_ref,
    pn_ref,
    on_ref,
    fp_ref,
    fo_ref,
    si_ref,
    pc_ref,
    sh_ref,
    oc_ref,
    f_ref,
    wp_ref,
    wo_ref,
    mf_ref,
    ms_ref,
    cp,
    co,
    rows,
    pair_in,
    half,
    zc,
    zin,
    zall,
    part,
    step_a,
    step_b,
    in_a,
    in_b,
    quarters,
    sq,
    sq_in,
    known,
    in_s,
    out_s,
    out_r,
):
    fs = lax.axis_index("fs")
    tp = lax.axis_index("tp")
    core = lax.rem(tp, 2)
    z = tp // 2
    z_count = tp_count // 2
    across_x = fs + 1 - 2 * lax.rem(fs, 2)
    across_y = lax.rem(fs + 2, 4)
    diagonal = 3 - fs
    partner = tp + 1 - 2 * core
    z_peers = [2 * lax.rem(z + o, z_count) + core for o in range(1, z_count)]
    tp_peers = [lax.rem(tp + o, tp_count) for o in range(1, tp_count)]
    to_x, to_y = {"fs": across_x}, {"fs": across_y}

    def send(src, dst, where, s, r):
        copy = pltpu.make_async_remote_copy(
            src_ref=src,
            dst_ref=dst,
            send_sem=out_s.at[s],
            recv_sem=out_r.at[r],
            device_id=where,
            device_id_type=MESH,
        )
        copy.start()
        return copy

    def whole(ref, s, r):
        return pltpu.make_async_remote_copy(
            src_ref=ref,
            dst_ref=ref,
            send_sem=out_s.at[s],
            recv_sem=out_r.at[r],
            device_id={"tp": partner},
            device_id_type=MESH,
        )

    def signal(sem, where):
        pl.semaphore_signal(sem, inc=1, device_id=where, device_id_type=MESH)

    barrier = pltpu.get_barrier_semaphore()

    @pl.when(core == 0)
    def _():
        signal(barrier, to_x)
        signal(barrier, to_y)

    @pl.when(core == 1)
    def _():
        signal(barrier, {"tp": partner})

    d_rows, width = cp.shape

    def share(n, start, stop, of=chunks):
        return pl.ds(start * n // of, (stop - start) * n // of)

    pairs = []
    for start, stop in ((0, 1), (1, chunks)):
        a, b = share(d_rows, start, stop), share(width, start, stop)
        pairs += [(wp_hbm.at[a, :], wp_ref.at[a, :]), (wo_hbm.at[b, :], wo_ref.at[b, :])]
    pairs += [
        (f_hbm, f_ref),
        (si_hbm, si_ref),
        (oc_hbm, oc_ref),
        (pc_hbm, pc_ref),
        (sh_hbm, sh_ref),
        (mf_hbm, mf_ref),
        (ms_hbm, ms_ref),
    ]
    loads = [pltpu.make_async_copy(a, b, in_s.at[i]) for i, (a, b) in enumerate(pairs)]
    for c in loads:
        c.start()

    loads[0].wait()
    cp[share(d_rows, 0, 1), :] = encode(wp_ref[share(d_rows, 0, 1), :], weight_gain, 4)

    @pl.when(core == 0)
    def _():
        pl.semaphore_wait(barrier, 3)
        signal(known.at[0], to_x)
        signal(known.at[0], to_y)

    @pl.when(core == 1)
    def _():
        pl.semaphore_wait(known.at[0], 1)
        for p in z_peers:
            signal(barrier, {"tp": p})

    for i in range(chunks):
        a, b = share(d_rows, i, i + 1), share(width, i, i + 1)
        if i == 1:
            loads[2].wait()
        if i:
            cp[a, :] = encode(wp_ref[a, :], weight_gain, 4)
        send(cp.at[a, :], gp_ref.at[0, a, :], to_x, 0, 0)
        if i < 2:
            loads[2 * i + 1].wait()
        co[b, :] = encode(wo_ref[b, :], weight_gain, 4)
        send(co.at[b, :], go_ref.at[1, b, :], to_y, 1, 1)
        if i == 0:

            @pl.when(core == 0)
            def _():
                pl.semaphore_wait(known.at[0], 2)
                signal(known.at[0], {"tp": partner})

    def more(start, stop):
        a, b = share(d_rows, start, stop, pieces), share(width, start, stop, pieces)
        send(co.at[b, :], go_ref.at[0, b, :], to_x, 0, 2)
        send(cp.at[a, :], gp_ref.at[1, a, :], to_y, 1, 3)

    cuts = (0, 2, 5, 8, 11, 16)
    more(cuts[0], cuts[1])
    for c in loads[4:7]:
        c.wait()

    tokens, feats = si_ref.shape
    own = pl.ds(pl.multiple_of(tp * feats, feats), feats)
    rows[0] = jnp.dot(si_ref[...], f_ref[0, own, :], preferred_element_type=jnp.float32)
    rows[1] = jnp.dot(oc_ref[...], f_ref[1, own, :], preferred_element_type=jnp.float32)
    paired = send(rows.at[1 - core], pair_in, {"tp": partner}, 2, 4)
    for c in loads[7:]:
        c.wait()
    rank = f_ref.shape[2]
    grams = [
        lax.dot_general(f_ref[k], f_ref[k], (((0,), (0,)), ((), ())), preferred_element_type=jnp.float32)
        for k in range(2)
    ]
    paired.wait_recv()
    half[...] = rows[core] + pair_in[...]
    piece = tokens // z_count

    def piece_of(i):
        return pl.ds(pl.multiple_of(i * piece, 8), piece)

    @pl.when(core == 1)
    def _():
        pl.semaphore_wait(barrier, z_count - 1)
        signal(known.at[1], {"tp": partner})

    @pl.when(core == 0)
    def _():
        pl.semaphore_wait(known.at[1], 1)

    scatter = []
    for i, p in enumerate(z_peers):
        pack(zc.at[i], half[piece_of(lax.rem(z + i + 1, z_count)), :])
        scatter.append(send(zc.at[i], zin.at[i], {"tp": p}, 3, 5 + i))
    total = half[piece_of(z), :]
    for i, c in enumerate(scatter):
        c.wait_recv()
        total = total + unpack(zin.at[i], piece)
    pack(zall.at[core, z], total)
    def hand(at, where, s, r):
        return send(zall.at[core, at], zall.at[core, at], where, s, r)

    gathers = [hand(z, {"tp": p}, 4, 8 + i) for i, p in enumerate(z_peers)]
    hand(z, {"tp": partner}, 5, 11)
    for i, c in enumerate(gathers):
        c.wait_recv()
        hand(lax.rem(z + z_count - 1 - i, z_count), {"tp": partner}, 5, 11)
    passed = whole(zall.at[core], 5, 11)
    passed.wait_recv()
    paired.wait_send()
    whole(zc, 3, 5).wait_send()
    whole(zc, 4, 5).wait_send()
    passed.wait_send()

    for k, right in enumerate((pc_ref, sh_ref)):
        for i in range(z_count):
            rows[k, i * piece : (i + 1) * piece, :] = unpack(zall.at[k, i], piece)
        left = two_parts(rows[k], 1)
        both = lax.dot_general(
            left, right[...], (((0,), (0,)), ((), ())), preferred_element_type=jnp.float32
        )
        both = both[:rank] + both[rank:]
        for j in range(4):
            part[k, j] = both[:, j * width // 4 : (j + 1) * width // 4]

    pack(step_a.at[0], part[0, across_x])
    pack(step_a.at[1], part[0, diagonal])
    pack(step_b.at[0], part[1, across_y])
    pack(step_b.at[1], part[1, diagonal])
    sums = [
        send(step_a.at[0:2], in_a.at[0:2], to_x, 3, 12),
        send(step_b.at[0:2], in_b.at[0:2], to_y, 4, 13),
    ]
    more(cuts[1], cuts[2])
    sums[0].wait_recv()
    pack(step_a.at[2], part[0, across_y] + unpack(in_a.at[1], rank))
    sums.append(send(step_a.at[2], in_a.at[2], to_y, 3, 14))
    sums[1].wait_recv()
    pack(step_b.at[2], part[1, across_x] + unpack(in_b.at[1], rank))
    sums.append(send(step_b.at[2], in_b.at[2], to_x, 4, 15))
    more(cuts[2], cuts[3])
    mine_a = part[0, fs] + unpack(in_a.at[0], rank)
    mine_b = part[1, fs] + unpack(in_b.at[0], rank)
    sums[2].wait_recv()
    pack(quarters.at[0, fs], mine_a + unpack(in_a.at[2], rank))

    def spread(k, at, where, r):
        return send(quarters.at[k, at], quarters.at[k, at], where, 5 + k, r)

    from_y = spread(0, fs, to_y, 16)
    spread(0, fs, to_x, 18)
    sums[3].wait_recv()
    pack(quarters.at[1, fs], mine_b + unpack(in_b.at[2], rank))
    from_x = spread(1, fs, to_x, 17)
    spread(1, fs, to_y, 18)
    more(cuts[3], cuts[4])
    from_y.wait_recv()
    spread(0, across_y, to_x, 18)
    from_x.wait_recv()
    spread(1, across_x, to_y, 18)
    more(cuts[4], cuts[5])
    whole(gp_ref.at[0], 0, 0).wait_recv()
    whole(go_ref.at[1], 1, 1).wait_recv()
    relays = []
    for i in range(chunks):
        a = share(d_rows, i, i + 1)
        relays += [
            send(gp_ref.at[0, a, :], gp_ref.at[2, a, :], to_y, 1, 20 + 2 * i),
            send(go_ref.at[1, :, a], go_ref.at[2, :, a], to_x, 0, 21 + 2 * i),
        ]
    whole(quarters.at[0], 5, 18).wait_recv()
    whole(step_a, 3, 12).wait_send()
    whole(step_b, 4, 13).wait_send()
    whole(step_a, 5, 12).wait_send()
    whole(step_b, 6, 13).wait_send()

    highest = lax.Precision.HIGHEST
    squares = []
    directions = []
    for k in range(2):
        small = jnp.concatenate([unpack(quarters.at[k, j], rank) for j in range(4)], axis=1)
        at = slice(k * rank, (k + 1) * rank)
        first = beta_first * mf_ref[at, :] + (1.0 - beta_first) * small
        second = beta_second * ms_ref[at, :] + (1.0 - beta_second) * small * small
        first_ref[at, :] = first
        second_ref[at, :] = second
        direction = first / (jnp.sqrt(second) + epsilon)
        directions.append(direction)
        seen = jnp.dot(grams[k], direction, preferred_element_type=jnp.float32, precision=highest)
        seen = jnp.sum(seen * direction, axis=0, keepdims=True)
        squares.append(jnp.sum(seen, axis=1, keepdims=True))
    row = lax.broadcasted_iota(jnp.int32, sq.shape, 0)
    sq[...] = jnp.where(row == 0, squares[0], squares[1])
    for i, p in enumerate(tp_peers):
        send(sq, sq_in.at[i], {"tp": p}, 2, 19)
    whole(sq_in, 2, 19).wait_recv()
    total = sq[...]
    for i in range(tp_count - 1):
        total = total + sq_in[i]
    scale = -learn_rate * lax.rsqrt(jnp.maximum(total, 0.0) / entries + epsilon)
    d0_ref[...] = two_parts(directions[0] * scale[0:1, 0:1], 0)
    d1_ref[...] = two_parts(jnp.transpose(directions[1] * scale[1:2, 0:1]), 1)
    whole(sq_in, 2, 19).wait_send()

    size = d_rows // chunks

    def block(slot, owner, proj_code, out_code, start=0, stop=chunks):
        def one(i, _):
            at = pl.ds(pl.multiple_of(i * size, size), size)
            there = pl.ds(pl.multiple_of(owner * d_rows + i * size, size), size)
            u = proj_step(f_ref[0, there, :], d0_ref)
            fp_ref[slot, at, :] = (decode(proj_code[at, :], weight_gain, 4) + u).astype(jnp.bfloat16)
            if slot == 0:
                pn_ref[at, :] = wp_ref[at, :] + u
            u = out_step(f_ref[1, there, :], d1_ref)
            fo_ref[slot, :, at] = (decode(out_code[:, at], weight_gain, 4) + u).astype(jnp.bfloat16)
            if slot == 0:
                on_ref[:, at] = wo_ref[:, at] + u
            return 0

        lax.fori_loop(start, stop, one, 0)

    block(0, fs, cp, co)
    whole(go_ref.at[0], 0, 2).wait_recv()
    block(1, across_x, gp_ref.at[0], go_ref.at[0])
    whole(gp_ref.at[1], 1, 3).wait_recv()
    block(2, across_y, gp_ref.at[1], go_ref.at[1])
    for i in range(chunks - 1):
        relays[2 * i].wait_recv()
        relays[2 * i + 1].wait_recv()
        block(3, diagonal, gp_ref.at[2], go_ref.at[2], i, i + 1)
    for c in relays[2 * chunks - 2 :]:
        c.wait_recv()
    whole(go_ref, 0, 0).wait_send()
    whole(gp_ref, 1, 1).wait_send()


def finish_kernel(
    me_ref, f_ref, d0, d1, gp, go, pn, on, fp, fo, mf, ms,
    pn_hbm, on_hbm, pc_hbm, oc_hbm, first_hbm, second_hbm, last_p, last_o, sems
):
    me = me_ref[0]
    d_rows = pn.shape[0]
    size = d_rows // chunks
    early = d_rows - size

    def span(owner, n=d_rows, start=0):
        return pl.ds(pl.multiple_of(owner * d_rows + start, size), n)

    pairs = [(pn, pn_hbm), (on, on_hbm), (mf, first_hbm), (ms, second_hbm)]
    for r, owner in enumerate((me, me ^ 1, me ^ 2)):
        pairs += [(fp.at[r], pc_hbm.at[span(owner), :]), (fo.at[r], oc_hbm.at[:, span(owner)])]
    pairs += [
        (fp.at[3, :early, :], pc_hbm.at[span(me ^ 3, early), :]),
        (fo.at[3, :, :early], oc_hbm.at[:, span(me ^ 3, early)]),
    ]
    copies = [pltpu.make_async_copy(a, b, sems.at[i]) for i, (a, b) in enumerate(pairs)]
    for c in copies:
        c.start()
    there = span(me ^ 3, size, early)
    u = proj_step(f_ref[0, there, :], d0)
    last_p[...] = (decode(gp[2, early:, :], weight_gain, 4) + u).astype(jnp.bfloat16)
    copies.append(pltpu.make_async_copy(last_p, pc_hbm.at[there, :], sems.at[len(copies)]))
    copies[-1].start()
    u = out_step(f_ref[1, there, :], d1)
    last_o[...] = (decode(go[2, :, early:], weight_gain, 4) + u).astype(jnp.bfloat16)
    copies.append(pltpu.make_async_copy(last_o, oc_hbm.at[:, there], sems.at[len(copies)]))
    copies[-1].start()
    for c in copies:
        c.wait()


def fast_body(si, pc, sh, oc, factors, w_proj, w_out, m1, m2):
    tp_count = lax.axis_size("tp")
    kinds, d_model, rank = factors.shape
    tokens = si.shape[0]
    width = pc.shape[1]
    d_rows = w_proj.shape[0]
    f32, bf16 = jnp.float32, jnp.bfloat16
    mf, ms = m1.reshape(2 * rank, width), m2.reshape(2 * rank, width)
    vm = pl.BlockSpec(memory_space=pltpu.VMEM)
    hbm = pl.BlockSpec(memory_space=pltpu.HBM)
    dma = lambda n: pltpu.SemaphoreType.DMA((n,))
    shape = jax.ShapeDtypeStruct
    peers = tp_count - 1
    z_count = tp_count // 2
    piece = tokens // z_count
    packed = -(-piece // pad_rows) * pad_rows + pad_rows
    quarter = width // 4
    args = (si, pc, sh, oc, factors, w_proj, w_out, mf, ms)
    held = tuple(pltpu.with_memory_space_constraint(a, pltpu.HBM) for a in args)
    first, second, d0, d1, gp, go, pn, on, fp, fo = pl.pallas_call(
        functools.partial(exchange_kernel, tp_count, float(d_model * width * tp_count)),
        out_shape=(
            pltpu.VMEM((2 * rank, width), f32),
            pltpu.VMEM((2 * rank, width), f32),
            pltpu.VMEM((2 * rank, width), bf16),
            pltpu.VMEM((width, 2 * rank), bf16),
            pltpu.VMEM((3, d_rows, width), bf16),
            pltpu.VMEM((3, width, d_rows), bf16),
            pltpu.VMEM((d_rows, width), f32),
            pltpu.VMEM((width, d_rows), f32),
            pltpu.VMEM((4, d_rows, width), bf16),
            pltpu.VMEM((4, width, d_rows), bf16),
        ),
        in_specs=[hbm] * 9,
        out_specs=(vm,) * 10,
        scratch_shapes=[pltpu.VMEM(a.shape, a.dtype) for a in args]
        + [
            pltpu.VMEM((d_rows, width), bf16),
            pltpu.VMEM((width, d_rows), bf16),
            pltpu.VMEM((2, tokens, rank), f32),
            pltpu.VMEM((tokens, rank), f32),
            pltpu.VMEM((tokens, rank), f32),
            pltpu.VMEM((z_count - 1, packed, rank), bf16),
            pltpu.VMEM((z_count - 1, packed, rank), bf16),
            pltpu.VMEM((2, z_count, packed, rank), bf16),
            pltpu.VMEM((2, 4, rank, quarter), f32),
            pltpu.VMEM((3, rank + pad_rows, quarter), bf16),
            pltpu.VMEM((3, rank + pad_rows, quarter), bf16),
            pltpu.VMEM((3, rank + pad_rows, quarter), bf16),
            pltpu.VMEM((3, rank + pad_rows, quarter), bf16),
            pltpu.VMEM((2, 4, rank + pad_rows, quarter), bf16),
            pltpu.VMEM((8, 128), f32),
            pltpu.VMEM((peers, 8, 128), f32),
            pltpu.SemaphoreType.REGULAR((2,)),
            dma(11),
            dma(7),
            dma(20 + 2 * chunks),
        ],
        compiler_params=pltpu.CompilerParams(
            collective_id=0, has_side_effects=True, vmem_limit_bytes=42 * MIB
        ),
        name="exchange",
    )(*held)

    me = lax.axis_index("fs").astype(jnp.int32).reshape(1)
    pn, on, pcopy, ocopy, first, second = pl.pallas_call(
        finish_kernel,
        in_specs=[pl.BlockSpec(memory_space=pltpu.SMEM)] + [vm] * 11,
        out_specs=[hbm] * 6,
        out_shape=(
            shape(w_proj.shape, f32),
            shape(w_out.shape, f32),
            shape((d_model, width), bf16),
            shape((width, d_model), bf16),
            shape((2 * rank, width), f32),
            shape((2 * rank, width), f32),
        ),
        scratch_shapes=[
            pltpu.VMEM((d_rows // chunks, width), bf16),
            pltpu.VMEM((width, d_rows // chunks), bf16),
            dma(14),
        ],
        compiler_params=pltpu.CompilerParams(vmem_limit_bytes=8 * MIB),
        name="finish",
    )(me, factors, d0, d1, gp, go, pn, on, fp, fo, first, second)
    return pn, on, pcopy, ocopy, first.reshape(m1.shape), second.reshape(m2.shape)


def over_tokens(left_rows, right_rows, precise):
    return lax.dot_general(
        left_rows,
        right_rows,
        (((0,), (0,)), ((), ())),
        preferred_element_type=jnp.float32,
        precision=precise,
    )


def body(
    saved_inputs,
    proj_cotangent,
    saved_hidden,
    out_cotangent,
    factors,
    w_proj,
    w_out,
    moment_first,
    moment_second,
):
    highest = lax.Precision.HIGHEST
    fs_count = lax.axis_size("fs")
    tp_count = lax.axis_size("tp")
    d_model = factors.shape[1]
    hidden_width = proj_cotangent.shape[1]
    fs_rows = d_model // fs_count
    tp_feats = saved_inputs.shape[1]
    own_rows = lax.dynamic_slice_in_dim(factors, lax.axis_index("fs") * fs_rows, fs_rows, 1).astype(
        jnp.float32
    )
    own_feats = lax.dynamic_slice_in_dim(factors, lax.axis_index("tp") * tp_feats, tp_feats, 1)
    proj_rows = jnp.dot(saved_inputs, own_feats[0], preferred_element_type=jnp.float32)
    out_rows = jnp.dot(out_cotangent, own_feats[1], preferred_element_type=jnp.float32)
    proj_rows, out_rows = lax.psum((proj_rows, out_rows), "tp")
    partial_sums = jnp.stack(
        [
            over_tokens(proj_rows, proj_cotangent.astype(jnp.float32), highest),
            over_tokens(out_rows, saved_hidden.astype(jnp.float32), highest),
        ]
    )
    small_grads = lax.psum(partial_sums, "fs")
    first_next = beta_first * moment_first + (1.0 - beta_first) * small_grads
    second_next = beta_second * moment_second + (1.0 - beta_second) * small_grads * small_grads
    direction = first_next / (jnp.sqrt(second_next) + epsilon)
    update_full = jnp.einsum("kdr,kre->kde", own_rows, direction, precision=highest)
    squares = lax.psum(jnp.sum(update_full * update_full, axis=(1, 2)), ("fs", "tp"))
    norm_scale = lax.rsqrt(squares / (d_model * hidden_width * tp_count) + epsilon)
    stepped = update_full * norm_scale[:, None, None]
    proj_next = w_proj - learn_rate * stepped[0]
    out_next = w_out - learn_rate * stepped[1].T
    proj_copy, out_copy = (
        lax.all_gather(proj_next.astype(jnp.bfloat16), "fs", axis=0, tiled=True),
        lax.all_gather(out_next.astype(jnp.bfloat16), "fs", axis=1, tiled=True),
    )
    return (proj_next, out_next, proj_copy, out_copy, first_next, second_next)


def solution(mesh):
    placed = (
        P("fs", "tp"),
        P("fs", "tp"),
        P("fs", "tp"),
        P("fs", "tp"),
        P(),
        P("fs", "tp"),
        P("tp", "fs"),
        P(None, None, "tp"),
        P(None, None, "tp"),
    )
    planned = fast_body if mesh.shape["fs"] == 4 and mesh.shape["tp"] == 8 else body
    return jax.shard_map(
        planned,
        mesh=mesh,
        in_specs=placed,
        out_specs=(
            P("fs", "tp"),
            P("tp", "fs"),
            P(None, "tp"),
            P("tp", None),
            P(None, None, "tp"),
            P(None, None, "tp"),
        ),
        check_vma=False,
    )
```

```python
import functools

import jax
import jax.numpy as jnp
from jax import lax
from jax.experimental import pallas as pl
from jax.experimental.pallas import tpu as pltpu
from jax.sharding import PartitionSpec as P

beta_first = 0.9
beta_second = 0.95
learn_rate = 0.02
epsilon = 1e-06
weight_rate = 1344.0
code_top = 200.0
chunks = 4
early = 1
pieces = 16
pad_rows = 16
MIB = 1024 * 1024
MESH = pl.DeviceIdType.MESH


def encode(x, gain, doublings):
    t = x * gain
    for _ in range(doublings):
        t = t * t
    return jnp.where(x < 0, -t, t).astype(jnp.bfloat16)


def decode(code, gain, doublings):
    v = code.astype(jnp.float32)
    size = jnp.exp2(jnp.log2(jnp.abs(v)) * (0.5**doublings)) * (1.0 / gain)
    return jnp.where(v < 0, -size, size)


def largest(x):
    top = jnp.max(jnp.max(jnp.abs(x), axis=0, keepdims=True), axis=1, keepdims=True)
    return jnp.maximum(top, 1e-30)


def two_parts(x, axis):
    high = x.astype(jnp.bfloat16)
    low = (x - high.astype(jnp.float32)).astype(jnp.bfloat16)
    return jnp.concatenate([high, low], axis=axis)


def proj_step(f, d0):
    return jnp.dot(jnp.concatenate([f, f], axis=1), d0[...], preferred_element_type=jnp.float32)


def out_step(f, d1):
    return lax.dot_general(
        d1[...],
        jnp.concatenate([f, f], axis=1),
        (((1,), (1,)), ((), ())),
        preferred_element_type=jnp.float32,
    )


def weight_code(x):
    return jnp.exp2(x * weight_rate).astype(jnp.bfloat16)


def weight_of(code):
    return jnp.log2(code.astype(jnp.float32)) * (1.0 / weight_rate)


def pack(ref, x):
    top = largest(x).astype(jnp.bfloat16)
    ref[: x.shape[0], :] = encode(x, code_top / top.astype(jnp.float32), 4)
    ref[ref.shape[0] - pad_rows :, :] = jnp.broadcast_to(top, (pad_rows, x.shape[1]))


def unpack(ref, n):
    top = ref[ref.shape[0] - pad_rows :, :][0:1, 0:1].astype(jnp.float32)
    return decode(ref[:n, :], code_top / top, 4)


def exchange_kernel(
    tp_count,
    entries,
    si_hbm,
    pc_hbm,
    sh_hbm,
    oc_hbm,
    f_hbm,
    wp_hbm,
    wo_hbm,
    mf_hbm,
    ms_hbm,
    first_ref,
    second_ref,
    d0_ref,
    d1_ref,
    gp_ref,
    go_ref,
    pn_ref,
    on_ref,
    fp_ref,
    fo_ref,
    f_ref,
    si_ref,
    pc_ref,
    sh_ref,
    oc_ref,
    wp_ref,
    wo_ref,
    mf_ref,
    ms_ref,
    cp,
    co,
    rows,
    pair_in,
    half,
    zc,
    zin,
    zall,
    part,
    step_a,
    step_b,
    in_a,
    in_b,
    quarters,
    sq,
    sq_in,
    known,
    in_s,
    out_s,
    out_r,
):
    fs = lax.axis_index("fs")
    tp = lax.axis_index("tp")
    core = lax.rem(tp, 2)
    z = tp // 2
    z_count = tp_count // 2
    across_x = fs + 1 - 2 * lax.rem(fs, 2)
    across_y = lax.rem(fs + 2, 4)
    diagonal = 3 - fs
    partner = tp + 1 - 2 * core
    z_peers = [2 * lax.rem(z + o, z_count) + core for o in range(1, z_count)]
    tp_peers = [lax.rem(tp + o, tp_count) for o in range(1, tp_count)]
    to_x, to_y = {"fs": across_x}, {"fs": across_y}

    def send(src, dst, where, s, r):
        copy = pltpu.make_async_remote_copy(
            src_ref=src,
            dst_ref=dst,
            send_sem=out_s.at[s],
            recv_sem=out_r.at[r],
            device_id=where,
            device_id_type=MESH,
        )
        copy.start()
        return copy

    def whole(ref, s, r):
        return pltpu.make_async_remote_copy(
            src_ref=ref,
            dst_ref=ref,
            send_sem=out_s.at[s],
            recv_sem=out_r.at[r],
            device_id={"tp": partner},
            device_id_type=MESH,
        )

    def signal(sem, where):
        pl.semaphore_signal(sem, inc=1, device_id=where, device_id_type=MESH)

    barrier = pltpu.get_barrier_semaphore()

    @pl.when(core == 0)
    def _():
        signal(barrier, to_x)
        signal(barrier, to_y)

    @pl.when(core == 1)
    def _():
        signal(barrier, {"tp": partner})

    d_rows, width = cp.shape

    def share(n, start, stop, of=chunks):
        return pl.ds(start * n // of, (stop - start) * n // of)

    spans = ((0, 2), (2, 6), (6, 10), (10, 15))
    pairs = []
    for start, stop in (spans[0], (spans[0][1], pieces)):
        a, b = share(d_rows, start, stop, pieces), share(width, start, stop, pieces)
        pairs += [(wp_hbm.at[a, :], wp_ref.at[a, :]), (wo_hbm.at[b, :], wo_ref.at[b, :])]
    pairs += [
        (f_hbm, f_ref),
        (si_hbm, si_ref),
        (oc_hbm, oc_ref),
        (pc_hbm, pc_ref),
        (sh_hbm, sh_ref),
        (mf_hbm, mf_ref),
        (ms_hbm, ms_ref),
    ]
    loads = [pltpu.make_async_copy(a, b, in_s.at[i]) for i, (a, b) in enumerate(pairs)]
    for c in loads[:4]:
        c.start()


    def encode_proj(start, stop):
        a = share(d_rows, start, stop, pieces)
        cp[a, :] = weight_code(wp_ref[a, :])

    def encode_out(start, stop):
        b = share(width, start, stop, pieces)
        co[b, :] = weight_code(wo_ref[b, :])

    def open_proj(start, stop):
        a = share(d_rows, start, stop, pieces)
        send(cp.at[a, :], gp_ref.at[0, a, :], to_x, 0, 0)

    def open_out(start, stop):
        b = share(width, start, stop, pieces)
        send(co.at[b, :], go_ref.at[1, b, :], to_y, 1, 1)

    loads[0].wait()
    encode_proj(*spans[0])
    loads[1].wait()
    encode_out(*spans[0])

    @pl.when(core == 0)
    def _():
        pl.semaphore_wait(barrier, 3)
        signal(known.at[0], to_x)
        signal(known.at[0], to_y)

    @pl.when(core == 1)
    def _():
        pl.semaphore_wait(known.at[0], 1)
        for p in z_peers:
            signal(barrier, {"tp": p})

    open_proj(*spans[0])
    open_out(*spans[0])
    for c in loads[4:]:
        c.start()

    @pl.when(core == 0)
    def _():
        pl.semaphore_wait(known.at[0], 2)
        signal(known.at[0], {"tp": partner})

    loads[2].wait()
    loads[3].wait()
    for start, stop in spans[1:]:
        encode_proj(start, stop)
        open_proj(start, stop)
        encode_out(start, stop)
        open_out(start, stop)
    last = spans[-1][1]
    encode_proj(last, pieces)
    encode_out(last, pieces)

    def more(start, stop):
        a, b = share(d_rows, start, stop, pieces), share(width, start, stop, pieces)
        send(co.at[b, :], go_ref.at[0, b, :], to_x, 0, 2)
        send(cp.at[a, :], gp_ref.at[1, a, :], to_y, 1, 3)

    cuts = (0, 1, 3, 5, 16)
    for c in loads[4:7]:
        c.wait()

    tokens, feats = si_ref.shape
    own = pl.ds(pl.multiple_of(tp * feats, feats), feats)
    rows[0] = jnp.dot(si_ref[...], f_ref[0, own, :], preferred_element_type=jnp.float32)
    rows[1] = jnp.dot(oc_ref[...], f_ref[1, own, :], preferred_element_type=jnp.float32)
    paired = send(rows.at[1 - core], pair_in, {"tp": partner}, 2, 4)
    for c in loads[7:]:
        c.wait()
    rank = f_ref.shape[2]
    grams = [
        lax.dot_general(f_ref[k], f_ref[k], (((0,), (0,)), ((), ())), preferred_element_type=jnp.float32)
        for k in range(2)
    ]
    paired.wait_recv()
    half[...] = rows[core] + pair_in[...]
    piece = tokens // z_count

    def piece_of(i):
        return pl.ds(pl.multiple_of(i * piece, 8), piece)

    @pl.when(core == 1)
    def _():
        pl.semaphore_wait(barrier, z_count - 1)
        signal(known.at[1], {"tp": partner})

    @pl.when(core == 0)
    def _():
        pl.semaphore_wait(known.at[1], 1)

    scatter = []
    for i, p in enumerate(z_peers):
        pack(zc.at[i], half[piece_of(lax.rem(z + i + 1, z_count)), :])
        scatter.append(send(zc.at[i], zin.at[i], {"tp": p}, 3, 5 + i))
    total = half[piece_of(z), :]
    for i, c in enumerate(scatter):
        c.wait_recv()
        total = total + unpack(zin.at[i], piece)
    pack(zall.at[core, z], total)
    def hand(at, where, s, r):
        return send(zall.at[core, at], zall.at[core, at], where, s, r)

    gathers = [hand(z, {"tp": p}, 4, 8 + i) for i, p in enumerate(z_peers)]
    hand(z, {"tp": partner}, 5, 11)
    for i, c in enumerate(gathers):
        c.wait_recv()
        hand(lax.rem(z + z_count - 1 - i, z_count), {"tp": partner}, 5, 11)
    passed = whole(zall.at[core], 5, 11)
    passed.wait_recv()
    paired.wait_send()
    whole(zc, 3, 5).wait_send()
    whole(zc, 4, 5).wait_send()
    passed.wait_send()

    for k, right in enumerate((pc_ref, sh_ref)):
        for i in range(z_count):
            rows[k, i * piece : (i + 1) * piece, :] = unpack(zall.at[k, i], piece)
        left = two_parts(rows[k], 1)
        both = lax.dot_general(
            left, right[...], (((0,), (0,)), ((), ())), preferred_element_type=jnp.float32
        )
        both = both[:rank] + both[rank:]
        for j in range(4):
            part[k, j] = both[:, j * width // 4 : (j + 1) * width // 4]

    pack(step_a.at[0], part[0, across_x])
    pack(step_a.at[1], part[0, diagonal])
    pack(step_b.at[0], part[1, across_y])
    pack(step_b.at[1], part[1, diagonal])
    sums = [
        send(step_a.at[0:2], in_a.at[0:2], to_x, 3, 12),
        send(step_b.at[0:2], in_b.at[0:2], to_y, 4, 13),
    ]
    open_proj(last, pieces)
    open_out(last, pieces)
    more(cuts[0], cuts[1])
    sums[0].wait_recv()
    pack(step_a.at[2], part[0, across_y] + unpack(in_a.at[1], rank))
    sums.append(send(step_a.at[2], in_a.at[2], to_y, 3, 14))
    sums[1].wait_recv()
    pack(step_b.at[2], part[1, across_x] + unpack(in_b.at[1], rank))
    sums.append(send(step_b.at[2], in_b.at[2], to_x, 4, 15))
    more(cuts[1], cuts[2])
    mine_a = part[0, fs] + unpack(in_a.at[0], rank)
    mine_b = part[1, fs] + unpack(in_b.at[0], rank)
    sums[2].wait_recv()
    pack(quarters.at[0, fs], mine_a + unpack(in_a.at[2], rank))

    def spread(k, at, where, r):
        return send(quarters.at[k, at], quarters.at[k, at], where, 5 + k, r)

    from_y = spread(0, fs, to_y, 16)
    spread(0, fs, to_x, 18)
    sums[3].wait_recv()
    pack(quarters.at[1, fs], mine_b + unpack(in_b.at[2], rank))
    from_x = spread(1, fs, to_x, 17)
    spread(1, fs, to_y, 18)
    more(cuts[2], cuts[3])
    from_y.wait_recv()
    spread(0, across_y, to_x, 18)
    from_x.wait_recv()
    spread(1, across_x, to_y, 18)
    more(cuts[3], cuts[4])
    whole(gp_ref.at[0], 0, 0).wait_recv()
    whole(go_ref.at[1], 1, 1).wait_recv()

    def relay(i):
        a = share(d_rows, i, i + 1)
        send(gp_ref.at[0, a, :], gp_ref.at[2, a, :], to_y, 1, 20 + 2 * i)
        send(go_ref.at[1, :, a], go_ref.at[2, :, a], to_x, 0, 21 + 2 * i)

    for i in range(early):
        relay(i)

    @pl.when(core == 1)
    def _():
        for i in range(early, chunks):
            relay(i)

    whole(quarters.at[0], 5, 18).wait_recv()
    whole(step_a, 3, 12).wait_send()
    whole(step_b, 4, 13).wait_send()
    whole(step_a, 5, 12).wait_send()
    whole(step_b, 6, 13).wait_send()

    highest = lax.Precision.HIGHEST
    squares = []
    directions = []
    for k in range(2):
        small = jnp.concatenate([unpack(quarters.at[k, j], rank) for j in range(4)], axis=1)
        at = slice(k * rank, (k + 1) * rank)
        first = beta_first * mf_ref[at, :] + (1.0 - beta_first) * small
        second = beta_second * ms_ref[at, :] + (1.0 - beta_second) * small * small
        first_ref[at, :] = first
        second_ref[at, :] = second
        direction = first / (jnp.sqrt(second) + epsilon)
        directions.append(direction)
        seen = jnp.dot(grams[k], direction, preferred_element_type=jnp.float32, precision=highest)
        seen = jnp.sum(seen * direction, axis=0, keepdims=True)
        squares.append(jnp.sum(seen, axis=1, keepdims=True))
    row = lax.broadcasted_iota(jnp.int32, sq.shape, 0)
    sq[...] = jnp.where(row == 0, squares[0], squares[1])
    for i, p in enumerate(tp_peers):
        send(sq, sq_in.at[i], {"tp": p}, 2, 19)
    whole(sq_in, 2, 19).wait_recv()
    total = sq[...]
    for i in range(tp_count - 1):
        total = total + sq_in[i]
    scale = -learn_rate * lax.rsqrt(jnp.maximum(total, 0.0) / entries + epsilon)
    d0_ref[...] = two_parts(directions[0] * scale[0:1, 0:1], 0)
    d1_ref[...] = two_parts(jnp.transpose(directions[1] * scale[1:2, 0:1]), 1)
    whole(sq_in, 2, 19).wait_send()

    size = d_rows // chunks

    def block(slot, owner, proj_code, out_code, start=0, stop=chunks):
        def one(i, _):
            at = pl.ds(pl.multiple_of(i * size, size), size)
            there = pl.ds(pl.multiple_of(owner * d_rows + i * size, size), size)
            u = proj_step(f_ref[0, there, :], d0_ref)
            fp_ref[slot, at, :] = (weight_of(proj_code[at, :]) + u).astype(jnp.bfloat16)
            if slot == 0:
                pn_ref[at, :] = wp_ref[at, :] + u
            u = out_step(f_ref[1, there, :], d1_ref)
            fo_ref[slot, :, at] = (weight_of(out_code[:, at]) + u).astype(jnp.bfloat16)
            if slot == 0:
                on_ref[:, at] = wo_ref[:, at] + u
            return 0

        lax.fori_loop(start, stop, one, 0)

    block(0, fs, cp, co)
    whole(go_ref.at[0], 0, 2).wait_recv()
    block(1, across_x, gp_ref.at[0], go_ref.at[0])
    whole(gp_ref.at[1], 1, 3).wait_recv()
    block(2, across_y, gp_ref.at[1], go_ref.at[1])

    def relayed(i):
        a = share(d_rows, i, i + 1)
        whole(gp_ref.at[2, a, :], 1, 20 + 2 * i).wait_recv()
        whole(go_ref.at[2, :, a], 0, 21 + 2 * i).wait_recv()
        block(3, diagonal, gp_ref.at[2], go_ref.at[2], i, i + 1)

    for i in range(early):
        relayed(i)
    whole(go_ref.at[0:2], 0, 0).wait_send()
    whole(gp_ref.at[0:2], 1, 1).wait_send()
    a = share(d_rows, 0, early)
    whole(gp_ref.at[2, a, :], 1, 0).wait_send()
    whole(go_ref.at[2, :, a], 0, 0).wait_send()

    @pl.when(core == 1)
    def _():
        for i in range(early, chunks):
            relayed(i)
        a = share(d_rows, early, chunks)
        whole(gp_ref.at[2, a, :], 1, 0).wait_send()
        whole(go_ref.at[2, :, a], 0, 0).wait_send()


def write_kernel(
    me_ref, core_ref, pn, on, fp, fo, mf, ms,
    pn_hbm, on_hbm, pc_hbm, oc_hbm, first_hbm, second_hbm, sems
):
    me = me_ref[0]
    d_rows = pn.shape[0]
    size = d_rows // chunks

    def span(owner, start=0, stop=chunks):
        return pl.ds(pl.multiple_of(owner * d_rows + start * size, size), (stop - start) * size)

    def diagonal(start, stop):
        a = pl.ds(start * size, (stop - start) * size)
        there = span(me ^ 3, start, stop)
        return [(fp.at[3, a, :], pc_hbm.at[there, :]), (fo.at[3, :, a], oc_hbm.at[:, there])]

    pairs = [(pn, pn_hbm), (on, on_hbm), (mf, first_hbm), (ms, second_hbm)]
    for r, owner in enumerate((me, me ^ 1, me ^ 2)):
        pairs += [(fp.at[r], pc_hbm.at[span(owner), :]), (fo.at[r], oc_hbm.at[:, span(owner)])]
    pairs += diagonal(0, early)
    copies = [pltpu.make_async_copy(a, b, sems.at[i]) for i, (a, b) in enumerate(pairs)]
    for c in copies:
        c.start()

    @pl.when(core_ref[0] == 1)
    def _():
        rest = [
            pltpu.make_async_copy(a, b, sems.at[len(copies) + i])
            for i, (a, b) in enumerate(diagonal(early, chunks))
        ]
        for c in rest:
            c.start()
        for c in rest:
            c.wait()

    for c in copies:
        c.wait()


def relay_kernel(f_ref, d0_ref, d1_ref, gp, go, lp_ref, lo_ref, fp_ref, fo_ref, out_s, out_r):
    fs = lax.axis_index("fs")
    core = lax.rem(lax.axis_index("tp"), 2)
    to_x = {"fs": fs + 1 - 2 * lax.rem(fs, 2)}
    to_y = {"fs": lax.rem(fs + 2, 4)}
    d_rows = gp.shape[1]
    size = d_rows // chunks

    @pl.when(core == 0)
    def _():
        barrier = pltpu.get_barrier_semaphore()
        for where in (to_x, to_y):
            pl.semaphore_signal(barrier, inc=1, device_id=where, device_id_type=MESH)
        pl.semaphore_wait(barrier, 2)
        copies = []
        for i in range(early, chunks):
            a, b = pl.ds(i * size, size), pl.ds((i - early) * size, size)
            for src, dst, where in (
                (gp.at[0, a, :], lp_ref.at[b, :], to_y),
                (go.at[1, :, a], lo_ref.at[:, b], to_x),
            ):
                c = pltpu.make_async_remote_copy(
                    src_ref=src,
                    dst_ref=dst,
                    send_sem=out_s.at[len(copies)],
                    recv_sem=out_r.at[len(copies)],
                    device_id=where,
                    device_id_type=MESH,
                )
                c.start()
                copies.append(c)
        for i in range(early, chunks - 1):
            at = slice((i - early) * size, (i - early + 1) * size)
            there = pl.ds(pl.multiple_of((3 - fs) * d_rows + i * size, size), size)
            copies[2 * (i - early)].wait_recv()
            u = proj_step(f_ref[0, there, :], d0_ref)
            fp_ref[at, :] = (weight_of(lp_ref[at, :]) + u).astype(jnp.bfloat16)
            copies[2 * (i - early) + 1].wait_recv()
            u = out_step(f_ref[1, there, :], d1_ref)
            fo_ref[:, at] = (weight_of(lo_ref[:, at]) + u).astype(jnp.bfloat16)
        for c in copies[-2:]:
            c.wait_recv()
        for c in copies:
            c.wait_send()


def finish_kernel(
    me_ref, core_ref, f_ref, d0, d1, lp, lo, fp, fo, pc_in, oc_in, pc_hbm, oc_hbm, last_p, last_o, sems
):
    me = me_ref[0]
    d_rows = f_ref.shape[1] // 4
    size = d_rows // chunks
    done = fp.shape[0]

    @pl.when(core_ref[0] == 0)
    def _():
        def span(start, n):
            return pl.ds(pl.multiple_of((me ^ 3) * d_rows + start, size), n)

        there = span(early * size, done)
        copies = [
            pltpu.make_async_copy(fp, pc_hbm.at[there, :], sems.at[0]),
            pltpu.make_async_copy(fo, oc_hbm.at[:, there], sems.at[1]),
        ]
        for c in copies:
            c.start()
        there = span(d_rows - size, size)
        u = proj_step(f_ref[0, there, :], d0)
        last_p[...] = (weight_of(lp[done:, :]) + u).astype(jnp.bfloat16)
        copies.append(pltpu.make_async_copy(last_p, pc_hbm.at[there, :], sems.at[2]))
        copies[-1].start()
        u = out_step(f_ref[1, there, :], d1)
        last_o[...] = (weight_of(lo[:, done:]) + u).astype(jnp.bfloat16)
        copies.append(pltpu.make_async_copy(last_o, oc_hbm.at[:, there], sems.at[3]))
        copies[-1].start()
        for c in copies:
            c.wait()


def fast_body(si, pc, sh, oc, factors, w_proj, w_out, m1, m2):
    tp_count = lax.axis_size("tp")
    kinds, d_model, rank = factors.shape
    tokens = si.shape[0]
    width = pc.shape[1]
    d_rows = w_proj.shape[0]
    f32, bf16 = jnp.float32, jnp.bfloat16
    mf, ms = m1.reshape(2 * rank, width), m2.reshape(2 * rank, width)
    vm = pl.BlockSpec(memory_space=pltpu.VMEM)
    hbm = pl.BlockSpec(memory_space=pltpu.HBM)
    dma = lambda n: pltpu.SemaphoreType.DMA((n,))
    shape = jax.ShapeDtypeStruct
    peers = tp_count - 1
    z_count = tp_count // 2
    piece = tokens // z_count
    packed = -(-piece // pad_rows) * pad_rows + pad_rows
    quarter = width // 4
    args = (si, pc, sh, oc, factors, w_proj, w_out, mf, ms)
    held = tuple(pltpu.with_memory_space_constraint(a, pltpu.HBM) for a in args)
    first, second, d0, d1, gp, go, pn, on, fp, fo, held_f = pl.pallas_call(
        functools.partial(exchange_kernel, tp_count, float(d_model * width * tp_count)),
        out_shape=(
            pltpu.VMEM((2 * rank, width), f32),
            pltpu.VMEM((2 * rank, width), f32),
            pltpu.VMEM((2 * rank, width), bf16),
            pltpu.VMEM((width, 2 * rank), bf16),
            pltpu.VMEM((3, d_rows, width), bf16),
            pltpu.VMEM((3, width, d_rows), bf16),
            pltpu.VMEM((d_rows, width), f32),
            pltpu.VMEM((width, d_rows), f32),
            pltpu.VMEM((4, d_rows, width), bf16),
            pltpu.VMEM((4, width, d_rows), bf16),
            pltpu.VMEM(factors.shape, bf16),
        ),
        in_specs=[hbm] * 9,
        out_specs=(vm,) * 11,
        scratch_shapes=[pltpu.VMEM(a.shape, a.dtype) for a in args if a is not factors]
        + [
            pltpu.VMEM((d_rows, width), bf16),
            pltpu.VMEM((width, d_rows), bf16),
            pltpu.VMEM((2, tokens, rank), f32),
            pltpu.VMEM((tokens, rank), f32),
            pltpu.VMEM((tokens, rank), f32),
            pltpu.VMEM((z_count - 1, packed, rank), bf16),
            pltpu.VMEM((z_count - 1, packed, rank), bf16),
            pltpu.VMEM((2, z_count, packed, rank), bf16),
            pltpu.VMEM((2, 4, rank, quarter), f32),
            pltpu.VMEM((3, rank + pad_rows, quarter), bf16),
            pltpu.VMEM((3, rank + pad_rows, quarter), bf16),
            pltpu.VMEM((3, rank + pad_rows, quarter), bf16),
            pltpu.VMEM((3, rank + pad_rows, quarter), bf16),
            pltpu.VMEM((2, 4, rank + pad_rows, quarter), bf16),
            pltpu.VMEM((8, 128), f32),
            pltpu.VMEM((peers, 8, 128), f32),
            pltpu.SemaphoreType.REGULAR((2,)),
            dma(11),
            dma(7),
            dma(20 + 2 * chunks),
        ],
        compiler_params=pltpu.CompilerParams(
            collective_id=0, has_side_effects=True, vmem_limit_bytes=42 * MIB
        ),
        name="exchange",
    )(*held)

    me = lax.axis_index("fs").astype(jnp.int32).reshape(1)
    core = lax.rem(lax.axis_index("tp"), 2).astype(jnp.int32).reshape(1)
    scalar = pl.BlockSpec(memory_space=pltpu.SMEM)
    pn, on, pcopy, ocopy, first, second = pl.pallas_call(
        write_kernel,
        in_specs=[scalar] * 2 + [vm] * 6,
        out_specs=[hbm] * 6,
        out_shape=(
            shape(w_proj.shape, f32),
            shape(w_out.shape, f32),
            shape((d_model, width), bf16),
            shape((width, d_model), bf16),
            shape((2 * rank, width), f32),
            shape((2 * rank, width), f32),
        ),
        scratch_shapes=[dma(14)],
        compiler_params=pltpu.CompilerParams(vmem_limit_bytes=4 * MIB),
        name="write",
    )(me, core, pn, on, fp, fo, first, second)

    size = d_rows // chunks
    late = chunks - early
    lp, lo, fp, fo = pl.pallas_call(
        relay_kernel,
        in_specs=[vm] * 5,
        out_specs=(vm,) * 4,
        out_shape=(
            pltpu.VMEM((late * size, width), bf16),
            pltpu.VMEM((width, late * size), bf16),
            pltpu.VMEM((late * size - size, width), bf16),
            pltpu.VMEM((width, late * size - size), bf16),
        ),
        scratch_shapes=[dma(2 * late), dma(2 * late)],
        compiler_params=pltpu.CompilerParams(
            collective_id=1, has_side_effects=True, vmem_limit_bytes=8 * MIB
        ),
        name="relay",
    )(held_f, d0, d1, gp, go)

    pcopy, ocopy = pl.pallas_call(
        finish_kernel,
        in_specs=[scalar] * 2 + [vm] * 7 + [hbm] * 2,
        out_specs=[hbm] * 2,
        out_shape=(shape(pcopy.shape, bf16), shape(ocopy.shape, bf16)),
        scratch_shapes=[pltpu.VMEM((size, width), bf16), pltpu.VMEM((width, size), bf16), dma(4)],
        input_output_aliases={9: 0, 10: 1},
        compiler_params=pltpu.CompilerParams(vmem_limit_bytes=4 * MIB),
        name="finish",
    )(me, core, held_f, d0, d1, lp, lo, fp, fo, pcopy, ocopy)
    return pn, on, pcopy, ocopy, first.reshape(m1.shape), second.reshape(m2.shape)


def over_tokens(left_rows, right_rows, precise):
    return lax.dot_general(
        left_rows,
        right_rows,
        (((0,), (0,)), ((), ())),
        preferred_element_type=jnp.float32,
        precision=precise,
    )


def body(
    saved_inputs,
    proj_cotangent,
    saved_hidden,
    out_cotangent,
    factors,
    w_proj,
    w_out,
    moment_first,
    moment_second,
):
    highest = lax.Precision.HIGHEST
    fs_count = lax.axis_size("fs")
    tp_count = lax.axis_size("tp")
    d_model = factors.shape[1]
    hidden_width = proj_cotangent.shape[1]
    fs_rows = d_model // fs_count
    tp_feats = saved_inputs.shape[1]
    own_rows = lax.dynamic_slice_in_dim(factors, lax.axis_index("fs") * fs_rows, fs_rows, 1).astype(
        jnp.float32
    )
    own_feats = lax.dynamic_slice_in_dim(factors, lax.axis_index("tp") * tp_feats, tp_feats, 1)
    proj_rows = jnp.dot(saved_inputs, own_feats[0], preferred_element_type=jnp.float32)
    out_rows = jnp.dot(out_cotangent, own_feats[1], preferred_element_type=jnp.float32)
    proj_rows, out_rows = lax.psum((proj_rows, out_rows), "tp")
    partial_sums = jnp.stack(
        [
            over_tokens(proj_rows, proj_cotangent.astype(jnp.float32), highest),
            over_tokens(out_rows, saved_hidden.astype(jnp.float32), highest),
        ]
    )
    small_grads = lax.psum(partial_sums, "fs")
    first_next = beta_first * moment_first + (1.0 - beta_first) * small_grads
    second_next = beta_second * moment_second + (1.0 - beta_second) * small_grads * small_grads
    direction = first_next / (jnp.sqrt(second_next) + epsilon)
    update_full = jnp.einsum("kdr,kre->kde", own_rows, direction, precision=highest)
    squares = lax.psum(jnp.sum(update_full * update_full, axis=(1, 2)), ("fs", "tp"))
    norm_scale = lax.rsqrt(squares / (d_model * hidden_width * tp_count) + epsilon)
    stepped = update_full * norm_scale[:, None, None]
    proj_next = w_proj - learn_rate * stepped[0]
    out_next = w_out - learn_rate * stepped[1].T
    proj_copy, out_copy = (
        lax.all_gather(proj_next.astype(jnp.bfloat16), "fs", axis=0, tiled=True),
        lax.all_gather(out_next.astype(jnp.bfloat16), "fs", axis=1, tiled=True),
    )
    return (proj_next, out_next, proj_copy, out_copy, first_next, second_next)


def solution(mesh):
    placed = (
        P("fs", "tp"),
        P("fs", "tp"),
        P("fs", "tp"),
        P("fs", "tp"),
        P(),
        P("fs", "tp"),
        P("tp", "fs"),
        P(None, None, "tp"),
        P(None, None, "tp"),
    )
    planned = fast_body if mesh.shape["fs"] == 4 and mesh.shape["tp"] == 8 else body
    return jax.shard_map(
        planned,
        mesh=mesh,
        in_specs=placed,
        out_specs=(
            P("fs", "tp"),
            P("tp", "fs"),
            P(None, "tp"),
            P("tp", None),
            P(None, None, "tp"),
            P(None, None, "tp"),
        ),
        check_vma=False,
    )
```

```python
import functools

import jax
import jax.numpy as jnp
from jax import lax
from jax.experimental import pallas as pl
from jax.experimental.pallas import tpu as pltpu
from jax.sharding import PartitionSpec as P

beta_first = 0.9
beta_second = 0.95
learn_rate = 0.02
epsilon = 1e-06
weight_rate = 1344.0
code_top = 200.0
chunks = 4
early = 1
late_cuts = (4, 8, 12, 14, 16)
pieces = 16
pad_rows = 8
lead = 1
MIB = 1024 * 1024
MESH = pl.DeviceIdType.MESH


def encode(x, gain, doublings):
    t = x * gain
    for _ in range(doublings):
        t = t * t
    return jnp.where(x < 0, -t, t).astype(jnp.bfloat16)


def decode(code, gain, doublings):
    v = code.astype(jnp.float32)
    size = jnp.exp2(jnp.log2(jnp.abs(v)) * (0.5**doublings)) * (1.0 / gain)
    return jnp.where(v < 0, -size, size)


def largest(x):
    top = jnp.max(jnp.max(jnp.abs(x), axis=0, keepdims=True), axis=1, keepdims=True)
    return jnp.maximum(top, 1e-30)


def two_parts(x, axis):
    high = x.astype(jnp.bfloat16)
    low = (x - high.astype(jnp.float32)).astype(jnp.bfloat16)
    return jnp.concatenate([high, low], axis=axis)


def proj_step(f, d0):
    return jnp.dot(jnp.concatenate([f, f], axis=1), d0[...], preferred_element_type=jnp.float32)


def out_step(f, d1):
    return lax.dot_general(
        d1[...],
        jnp.concatenate([f, f], axis=1),
        (((1,), (1,)), ((), ())),
        preferred_element_type=jnp.float32,
    )


def weight_code(x):
    return jnp.exp2(x * weight_rate).astype(jnp.bfloat16)


def weight_of(code):
    return jnp.log2(code.astype(jnp.float32)) * (1.0 / weight_rate)


def pack(ref, x):
    top = largest(x).astype(jnp.bfloat16)
    ref[: x.shape[0], :] = encode(x, code_top / top.astype(jnp.float32), 4)
    ref[ref.shape[0] - pad_rows :, :] = jnp.broadcast_to(top, (pad_rows, x.shape[1]))


def unpack(ref, n):
    top = ref[ref.shape[0] - pad_rows :, :][0:1, 0:1].astype(jnp.float32)
    return decode(ref[:n, :], code_top / top, 4)


def exchange_kernel(
    tp_count,
    entries,
    si_hbm,
    pc_hbm,
    sh_hbm,
    oc_hbm,
    f_hbm,
    wp_hbm,
    wo_hbm,
    mf_hbm,
    ms_hbm,
    first_ref,
    second_ref,
    d0_ref,
    d1_ref,
    gp_ref,
    go_ref,
    pn_ref,
    on_ref,
    fp_ref,
    fo_ref,
    f_ref,
    si_ref,
    pc_ref,
    sh_ref,
    oc_ref,
    wp_ref,
    wo_ref,
    mf_ref,
    ms_ref,
    cp,
    co,
    rows,
    pair_in,
    half,
    zc,
    zin,
    zall,
    part,
    pair_a,
    pair_b,
    pair_in_a,
    pair_in_b,
    step_a,
    step_b,
    in_a,
    in_b,
    quarters,
    sq,
    sq_in,
    known,
    in_s,
    out_s,
    out_r,
):
    fs = lax.axis_index("fs")
    tp = lax.axis_index("tp")
    core = lax.rem(tp, 2)
    z = tp // 2
    z_count = tp_count // 2
    across_x = fs + 1 - 2 * lax.rem(fs, 2)
    across_y = lax.rem(fs + 2, 4)
    diagonal = 3 - fs
    partner = tp + 1 - 2 * core
    z_peers = [2 * lax.rem(z + o, z_count) + core for o in range(1, z_count)]
    tp_peers = [lax.rem(tp + o, tp_count) for o in range(1, tp_count)]
    to_x, to_y = {"fs": across_x}, {"fs": across_y}

    def send(src, dst, where, s, r):
        copy = pltpu.make_async_remote_copy(
            src_ref=src,
            dst_ref=dst,
            send_sem=out_s.at[s],
            recv_sem=out_r.at[r],
            device_id=where,
            device_id_type=MESH,
        )
        copy.start()
        return copy

    def whole(ref, s, r):
        return pltpu.make_async_remote_copy(
            src_ref=ref,
            dst_ref=ref,
            send_sem=out_s.at[s],
            recv_sem=out_r.at[r],
            device_id={"tp": partner},
            device_id_type=MESH,
        )

    def signal(sem, where):
        pl.semaphore_signal(sem, inc=1, device_id=where, device_id_type=MESH)

    barrier = pltpu.get_barrier_semaphore()

    @pl.when(core == lead)
    def _():
        signal(barrier, to_x)
        signal(barrier, to_y)

    @pl.when(core != lead)
    def _():
        signal(barrier, {"tp": partner})

    d_rows, width = cp.shape

    def share(n, start, stop, of=chunks):
        return pl.ds(start * n // of, (stop - start) * n // of)

    spans = ((0, 1), (1, 5), (5, 10), (10, 15))
    pairs = []
    for start, stop in (spans[0], spans[1], (spans[1][1], pieces)):
        a, b = share(d_rows, start, stop, pieces), share(width, start, stop, pieces)
        pairs += [(wp_hbm.at[a, :], wp_ref.at[a, :]), (wo_hbm.at[b, :], wo_ref.at[b, :])]
    pairs += [
        (f_hbm, f_ref),
        (si_hbm, si_ref),
        (oc_hbm, oc_ref),
        (pc_hbm, pc_ref),
        (sh_hbm, sh_ref),
        (mf_hbm, mf_ref),
        (ms_hbm, ms_ref),
    ]
    loads = [pltpu.make_async_copy(a, b, in_s.at[i]) for i, (a, b) in enumerate(pairs)]
    for c in loads[:4]:
        c.start()


    def encode_proj(start, stop):
        a = share(d_rows, start, stop, pieces)
        cp[a, :] = weight_code(wp_ref[a, :])

    def encode_out(start, stop):
        b = share(width, start, stop, pieces)
        co[b, :] = weight_code(wo_ref[b, :])

    def open_proj(start, stop):
        a = share(d_rows, start, stop, pieces)
        send(cp.at[a, :], gp_ref.at[0, a, :], to_x, 0, 0)

    def open_out(start, stop):
        b = share(width, start, stop, pieces)
        send(co.at[b, :], go_ref.at[1, b, :], to_y, 1, 1)

    loads[0].wait()
    encode_proj(*spans[0])
    loads[1].wait()
    encode_out(*spans[0])

    @pl.when(core == lead)
    def _():
        pl.semaphore_wait(barrier, 3)
        signal(known.at[0], to_x)
        signal(known.at[0], to_y)

    @pl.when(core != lead)
    def _():
        pl.semaphore_wait(known.at[0], 1)
        for p in z_peers:
            signal(barrier, {"tp": p})

    open_proj(*spans[0])
    open_out(*spans[0])
    for c in loads[4:]:
        c.start()
    for n, (start, stop) in enumerate(spans[1:]):
        if n < 2:
            loads[2 * n + 2].wait()
        encode_proj(start, stop)
        open_proj(start, stop)
        if n < 2:
            loads[2 * n + 3].wait()
        encode_out(start, stop)
        open_out(start, stop)
        if n == 0:

            @pl.when(core == lead)
            def _():
                pl.semaphore_wait(known.at[0], 2)
                signal(known.at[0], {"tp": partner})

    last = spans[-1][1]
    encode_proj(last, pieces)
    encode_out(last, pieces)

    def more(start, stop):
        a, b = share(d_rows, start, stop, pieces), share(width, start, stop, pieces)
        send(co.at[b, :], go_ref.at[0, b, :], to_x, 0, 2)
        send(cp.at[a, :], gp_ref.at[1, a, :], to_y, 1, 3)

    cuts = (0, 1, 3, 5, 16)
    for c in loads[6:9]:
        c.wait()

    tokens, feats = si_ref.shape
    own = pl.ds(pl.multiple_of(tp * feats, feats), feats)
    rows[0] = jnp.dot(si_ref[...], f_ref[0, own, :], preferred_element_type=jnp.float32)
    rows[1] = jnp.dot(oc_ref[...], f_ref[1, own, :], preferred_element_type=jnp.float32)
    paired = send(rows.at[1 - core], pair_in, {"tp": partner}, 2, 4)
    for c in loads[9:]:
        c.wait()
    rank = f_ref.shape[2]
    grams = [
        lax.dot_general(f_ref[k], f_ref[k], (((0,), (0,)), ((), ())), preferred_element_type=jnp.float32)
        for k in range(2)
    ]
    paired.wait_recv()
    half[...] = rows[core] + pair_in[...]
    piece = tokens // z_count

    def piece_of(i):
        return pl.ds(pl.multiple_of(i * piece, 8), piece)

    @pl.when(core != lead)
    def _():
        pl.semaphore_wait(barrier, z_count - 1)
        signal(known.at[1], {"tp": partner})

    @pl.when(core == lead)
    def _():
        pl.semaphore_wait(known.at[1], 1)

    scatter = []
    for i, p in enumerate(z_peers):
        pack(zc.at[i], half[piece_of(lax.rem(z + i + 1, z_count)), :])
        scatter.append(send(zc.at[i], zin.at[i], {"tp": p}, 3, 5 + i))
    total = half[piece_of(z), :]
    for i, c in enumerate(scatter):
        c.wait_recv()
        total = total + unpack(zin.at[i], piece)
    pack(zall.at[core, z], total)
    def hand(at, where, s, r):
        return send(zall.at[core, at], zall.at[core, at], where, s, r)

    gathers = [hand(z, {"tp": p}, 4, 8 + i) for i, p in enumerate(z_peers)]
    hand(z, {"tp": partner}, 5, 11)
    for i, c in enumerate(gathers):
        c.wait_recv()
        hand(lax.rem(z + z_count - 1 - i, z_count), {"tp": partner}, 5, 11)
    passed = whole(zall.at[core], 5, 11)
    passed.wait_recv()
    paired.wait_send()
    whole(zc, 3, 5).wait_send()
    whole(zc, 4, 5).wait_send()
    passed.wait_send()

    for k, right in enumerate((pc_ref, sh_ref)):
        for i in range(z_count):
            rows[k, i * piece : (i + 1) * piece, :] = unpack(zall.at[k, i], piece)
        left = two_parts(rows[k], 1)
        both = lax.dot_general(
            left, right[...], (((0,), (0,)), ((), ())), preferred_element_type=jnp.float32
        )
        both = both[:rank] + both[rank:]
        for j in range(4):
            part[k, j] = both[:, j * width // 4 : (j + 1) * width // 4]

    pack(pair_a, jnp.concatenate([part[0, across_x], part[0, diagonal]], axis=0))
    pack(pair_b, jnp.concatenate([part[1, across_y], part[1, diagonal]], axis=0))
    sums = [
        send(pair_a, pair_in_a, to_x, 3, 12),
        send(pair_b, pair_in_b, to_y, 4, 13),
    ]
    open_proj(last, pieces)
    open_out(last, pieces)
    more(cuts[0], cuts[1])
    sums[0].wait_recv()
    got_a = unpack(pair_in_a, 2 * rank)
    pack(step_a, part[0, across_y] + got_a[rank:])
    sums.append(send(step_a, in_a, to_y, 7, 14))
    sums[1].wait_recv()
    got_b = unpack(pair_in_b, 2 * rank)
    pack(step_b, part[1, across_x] + got_b[rank:])
    sums.append(send(step_b, in_b, to_x, 8, 15))
    more(cuts[1], cuts[2])
    sums[2].wait_recv()
    pack(quarters.at[0, fs], part[0, fs] + got_a[:rank] + unpack(in_a, rank))

    def spread(k, at, where, r):
        return send(quarters.at[k, at], quarters.at[k, at], where, 5 + k, r)

    from_y = spread(0, fs, to_y, 16)
    spread(0, fs, to_x, 18)
    sums[3].wait_recv()
    pack(quarters.at[1, fs], part[1, fs] + got_b[:rank] + unpack(in_b, rank))
    from_x = spread(1, fs, to_x, 17)
    spread(1, fs, to_y, 18)
    more(cuts[2], cuts[3])
    from_y.wait_recv()
    spread(0, across_y, to_x, 18)
    from_x.wait_recv()
    spread(1, across_x, to_y, 18)
    more(cuts[3], cuts[4])
    whole(gp_ref.at[0], 0, 0).wait_recv()
    whole(go_ref.at[1], 1, 1).wait_recv()

    def relay(i):
        a = share(d_rows, i, i + 1)
        send(gp_ref.at[0, a, :], gp_ref.at[2, a, :], to_y, 1, 20 + 2 * i)
        send(go_ref.at[1, :, a], go_ref.at[2, :, a], to_x, 0, 21 + 2 * i)

    for i in range(early):
        relay(i)

    @pl.when(core != lead)
    def _():
        for i in range(early, chunks):
            relay(i)

    whole(quarters.at[0], 5, 18).wait_recv()
    for c in sums:
        c.wait_send()
    whole(quarters.at[0, 0:3], 5, 12).wait_send()
    whole(quarters.at[1, 0:3], 6, 13).wait_send()

    highest = lax.Precision.HIGHEST
    squares = []
    directions = []
    for k in range(2):
        small = jnp.concatenate([unpack(quarters.at[k, j], rank) for j in range(4)], axis=1)
        at = slice(k * rank, (k + 1) * rank)
        first = beta_first * mf_ref[at, :] + (1.0 - beta_first) * small
        second = beta_second * ms_ref[at, :] + (1.0 - beta_second) * small * small
        first_ref[at, :] = first
        second_ref[at, :] = second
        direction = first / (jnp.sqrt(second) + epsilon)
        directions.append(direction)
        seen = jnp.dot(grams[k], direction, preferred_element_type=jnp.float32, precision=highest)
        seen = jnp.sum(seen * direction, axis=0, keepdims=True)
        squares.append(jnp.sum(seen, axis=1, keepdims=True))
    row = lax.broadcasted_iota(jnp.int32, sq.shape, 0)
    sq[...] = jnp.where(row == 0, squares[0], squares[1])
    for i, p in enumerate(tp_peers):
        send(sq, sq_in.at[i], {"tp": p}, 2, 19)
    whole(sq_in, 2, 19).wait_recv()
    total = sq[...]
    for i in range(tp_count - 1):
        total = total + sq_in[i]
    scale = -learn_rate * lax.rsqrt(jnp.maximum(total, 0.0) / entries + epsilon)
    d0_ref[...] = two_parts(directions[0] * scale[0:1, 0:1], 0)
    d1_ref[...] = two_parts(jnp.transpose(directions[1] * scale[1:2, 0:1]), 1)
    whole(sq_in, 2, 19).wait_send()

    size = d_rows // chunks

    def block(slot, owner, proj_code, out_code, start=0, stop=chunks):
        def one(i, _):
            at = pl.ds(pl.multiple_of(i * size, size), size)
            there = pl.ds(pl.multiple_of(owner * d_rows + i * size, size), size)
            u = proj_step(f_ref[0, there, :], d0_ref)
            fp_ref[slot, at, :] = (weight_of(proj_code[at, :]) + u).astype(jnp.bfloat16)
            if slot == 0:
                pn_ref[at, :] = wp_ref[at, :] + u
            u = out_step(f_ref[1, there, :], d1_ref)
            fo_ref[slot, :, at] = (weight_of(out_code[:, at]) + u).astype(jnp.bfloat16)
            if slot == 0:
                on_ref[:, at] = wo_ref[:, at] + u
            return 0

        lax.fori_loop(start, stop, one, 0)

    block(0, fs, cp, co)
    whole(go_ref.at[0], 0, 2).wait_recv()
    block(1, across_x, gp_ref.at[0], go_ref.at[0])
    whole(gp_ref.at[1], 1, 3).wait_recv()
    block(2, across_y, gp_ref.at[1], go_ref.at[1])

    def relayed(i):
        a = share(d_rows, i, i + 1)
        whole(gp_ref.at[2, a, :], 1, 20 + 2 * i).wait_recv()
        whole(go_ref.at[2, :, a], 0, 21 + 2 * i).wait_recv()
        block(3, diagonal, gp_ref.at[2], go_ref.at[2], i, i + 1)

    for i in range(early):
        relayed(i)
    whole(go_ref.at[0:2], 0, 0).wait_send()
    whole(gp_ref.at[0:2], 1, 1).wait_send()
    a = share(d_rows, 0, early)
    whole(gp_ref.at[2, a, :], 1, 0).wait_send()
    whole(go_ref.at[2, :, a], 0, 0).wait_send()

    @pl.when(core != lead)
    def _():
        for i in range(early, chunks):
            relayed(i)
        a = share(d_rows, early, chunks)
        whole(gp_ref.at[2, a, :], 1, 0).wait_send()
        whole(go_ref.at[2, :, a], 0, 0).wait_send()


def write_kernel(
    pn, on, fp, fo, mf, ms,
    pn_hbm, on_hbm, pc_hbm, oc_hbm, first_hbm, second_hbm, written, sems
):
    me = lax.axis_index("fs")
    core = lax.rem(lax.axis_index("tp"), 2)
    d_rows = pn.shape[0]
    size = d_rows // chunks

    def span(owner, start=0, stop=chunks):
        return pl.ds(pl.multiple_of(owner * d_rows + start * size, size), (stop - start) * size)

    def diagonal(start, stop):
        a = pl.ds(start * size, (stop - start) * size)
        there = span(3 - me, start, stop)
        return [(fp.at[3, a, :], pc_hbm.at[there, :]), (fo.at[3, :, a], oc_hbm.at[:, there])]

    pairs = [(pn, pn_hbm), (on, on_hbm), (mf, first_hbm), (ms, second_hbm)]
    for r, owner in enumerate((me, me + 1 - 2 * lax.rem(me, 2), lax.rem(me + 2, 4))):
        pairs += [(fp.at[r], pc_hbm.at[span(owner), :]), (fo.at[r], oc_hbm.at[:, span(owner)])]
    pairs += diagonal(0, early)
    copies = [pltpu.make_async_copy(a, b, sems.at[i]) for i, (a, b) in enumerate(pairs)]
    for c in copies:
        c.start()

    @pl.when(core != lead)
    def _():
        rest = [
            pltpu.make_async_copy(a, b, sems.at[len(copies) + i])
            for i, (a, b) in enumerate(diagonal(early, chunks))
        ]
        for c in rest:
            c.start()
        for c in rest:
            c.wait()

    for c in copies:
        c.wait()
    written[...] = jnp.zeros_like(written)


def relay_kernel(written, f_ref, d0_ref, d1_ref, gp, go, lp_ref, lo_ref, fp_ref, fo_ref, out_s, out_r):
    fs = lax.axis_index("fs")
    core = lax.rem(lax.axis_index("tp"), 2)
    to_x = {"fs": fs + 1 - 2 * lax.rem(fs, 2)}
    to_y = {"fs": lax.rem(fs + 2, 4)}
    d_rows = gp.shape[1]
    first = early * d_rows // chunks

    @pl.when(core == lead)
    def _():
        barrier = pltpu.get_barrier_semaphore()
        for where in (to_x, to_y):
            pl.semaphore_signal(barrier, inc=1, device_id=where, device_id_type=MESH)
        pl.semaphore_wait(barrier, 2)
        copies = []
        for start, stop in zip(late_cuts[:-1], late_cuts[1:]):
            start, stop = start * d_rows // pieces, stop * d_rows // pieces
            a, b = pl.ds(start, stop - start), pl.ds(start - first, stop - start)
            for src, dst, where in (
                (gp.at[0, a, :], lp_ref.at[b, :], to_y),
                (go.at[1, :, a], lo_ref.at[:, b], to_x),
            ):
                c = pltpu.make_async_remote_copy(
                    src_ref=src,
                    dst_ref=dst,
                    send_sem=out_s.at[len(copies)],
                    recv_sem=out_r.at[len(copies)],
                    device_id=where,
                    device_id_type=MESH,
                )
                c.start()
                copies.append(c)
        for i, (start, stop) in enumerate(zip(late_cuts[:-2], late_cuts[1:-1])):
            start, stop = start * d_rows // pieces, stop * d_rows // pieces
            at = slice(start - first, stop - first)
            there = pl.ds(pl.multiple_of((3 - fs) * d_rows + start, d_rows // pieces), stop - start)
            copies[2 * i].wait_recv()
            u = proj_step(f_ref[0, there, :], d0_ref)
            fp_ref[at, :] = (weight_of(lp_ref[at, :]) + u).astype(jnp.bfloat16)
            copies[2 * i + 1].wait_recv()
            u = out_step(f_ref[1, there, :], d1_ref)
            fo_ref[:, at] = (weight_of(lo_ref[:, at]) + u).astype(jnp.bfloat16)
        for c in copies[-2:]:
            c.wait_recv()
        for c in copies:
            c.wait_send()


def finish_kernel(
    f_ref, d0, d1, lp, lo, fp, fo, pc_in, oc_in, pc_hbm, oc_hbm, last_p, last_o, sems
):
    me = lax.axis_index("fs")
    core = lax.rem(lax.axis_index("tp"), 2)
    d_rows = f_ref.shape[1] // 4
    done, size = fp.shape[0], last_p.shape[0]

    @pl.when(core == lead)
    def _():
        def span(start, n):
            return pl.ds(pl.multiple_of((3 - me) * d_rows + start, size), n)

        there = span(d_rows - size - done, done)
        copies = [
            pltpu.make_async_copy(fp, pc_hbm.at[there, :], sems.at[0]),
            pltpu.make_async_copy(fo, oc_hbm.at[:, there], sems.at[1]),
        ]
        for c in copies:
            c.start()
        there = span(d_rows - size, size)
        u = proj_step(f_ref[0, there, :], d0)
        last_p[...] = (weight_of(lp[done:, :]) + u).astype(jnp.bfloat16)
        copies.append(pltpu.make_async_copy(last_p, pc_hbm.at[there, :], sems.at[2]))
        copies[-1].start()
        u = out_step(f_ref[1, there, :], d1)
        last_o[...] = (weight_of(lo[:, done:]) + u).astype(jnp.bfloat16)
        copies.append(pltpu.make_async_copy(last_o, oc_hbm.at[:, there], sems.at[3]))
        copies[-1].start()
        for i, c in enumerate(copies):
            c.wait()


def fast_body(si, pc, sh, oc, factors, w_proj, w_out, m1, m2):
    tp_count = lax.axis_size("tp")
    kinds, d_model, rank = factors.shape
    tokens = si.shape[0]
    width = pc.shape[1]
    d_rows = w_proj.shape[0]
    f32, bf16 = jnp.float32, jnp.bfloat16
    mf, ms = m1.reshape(2 * rank, width), m2.reshape(2 * rank, width)
    vm = pl.BlockSpec(memory_space=pltpu.VMEM)
    hbm = pl.BlockSpec(memory_space=pltpu.HBM)
    dma = lambda n: pltpu.SemaphoreType.DMA((n,))
    shape = jax.ShapeDtypeStruct
    peers = tp_count - 1
    z_count = tp_count // 2
    piece = tokens // z_count
    packed = -(-piece // pad_rows) * pad_rows + pad_rows
    quarter = width // 4
    args = (si, pc, sh, oc, factors, w_proj, w_out, mf, ms)
    held = tuple(pltpu.with_memory_space_constraint(a, pltpu.HBM) for a in args)
    first, second, d0, d1, gp, go, pn, on, fp, fo, held_f = pl.pallas_call(
        functools.partial(exchange_kernel, tp_count, float(d_model * width * tp_count)),
        out_shape=(
            pltpu.VMEM((2 * rank, width), f32),
            pltpu.VMEM((2 * rank, width), f32),
            pltpu.VMEM((2 * rank, width), bf16),
            pltpu.VMEM((width, 2 * rank), bf16),
            pltpu.VMEM((3, d_rows, width), bf16),
            pltpu.VMEM((3, width, d_rows), bf16),
            pltpu.VMEM((d_rows, width), f32),
            pltpu.VMEM((width, d_rows), f32),
            pltpu.VMEM((4, d_rows, width), bf16),
            pltpu.VMEM((4, width, d_rows), bf16),
            pltpu.VMEM(factors.shape, bf16),
        ),
        in_specs=[hbm] * 9,
        out_specs=(vm,) * 11,
        scratch_shapes=[pltpu.VMEM(a.shape, a.dtype) for a in args if a is not factors]
        + [
            pltpu.VMEM((d_rows, width), bf16),
            pltpu.VMEM((width, d_rows), bf16),
            pltpu.VMEM((2, tokens, rank), f32),
            pltpu.VMEM((tokens, rank), f32),
            pltpu.VMEM((tokens, rank), f32),
            pltpu.VMEM((z_count - 1, packed, rank), bf16),
            pltpu.VMEM((z_count - 1, packed, rank), bf16),
            pltpu.VMEM((2, z_count, packed, rank), bf16),
            pltpu.VMEM((2, 4, rank, quarter), f32),
            pltpu.VMEM((2 * rank + pad_rows, quarter), bf16),
            pltpu.VMEM((2 * rank + pad_rows, quarter), bf16),
            pltpu.VMEM((2 * rank + pad_rows, quarter), bf16),
            pltpu.VMEM((2 * rank + pad_rows, quarter), bf16),
            pltpu.VMEM((rank + pad_rows, quarter), bf16),
            pltpu.VMEM((rank + pad_rows, quarter), bf16),
            pltpu.VMEM((rank + pad_rows, quarter), bf16),
            pltpu.VMEM((rank + pad_rows, quarter), bf16),
            pltpu.VMEM((2, 4, rank + pad_rows, quarter), bf16),
            pltpu.VMEM((8, 128), f32),
            pltpu.VMEM((peers, 8, 128), f32),
            pltpu.SemaphoreType.REGULAR((2,)),
            dma(13),
            dma(9),
            dma(20 + 2 * chunks),
        ],
        compiler_params=pltpu.CompilerParams(
            collective_id=0, has_side_effects=True, vmem_limit_bytes=42 * MIB
        ),
        name="exchange",
    )(*held)

    pn, on, pcopy, ocopy, first, second, written = pl.pallas_call(
        write_kernel,
        in_specs=[vm] * 6,
        out_specs=[hbm] * 6 + [vm],
        out_shape=(
            shape(w_proj.shape, f32),
            shape(w_out.shape, f32),
            shape((d_model, width), bf16),
            shape((width, d_model), bf16),
            shape((2 * rank, width), f32),
            shape((2 * rank, width), f32),
            pltpu.VMEM((8, 128), f32),
        ),
        scratch_shapes=[dma(14)],
        compiler_params=pltpu.CompilerParams(vmem_limit_bytes=4 * MIB),
        name="write",
    )(pn, on, fp, fo, first, second)

    size = d_rows * (late_cuts[-1] - late_cuts[-2]) // pieces
    rest = d_rows - early * d_rows // chunks
    count = 2 * len(late_cuts) - 2
    lp, lo, fp, fo = pl.pallas_call(
        relay_kernel,
        in_specs=[vm] * 6,
        out_specs=(vm,) * 4,
        out_shape=(
            pltpu.VMEM((rest, width), bf16),
            pltpu.VMEM((width, rest), bf16),
            pltpu.VMEM((rest - size, width), bf16),
            pltpu.VMEM((width, rest - size), bf16),
        ),
        scratch_shapes=[dma(count), dma(count)],
        compiler_params=pltpu.CompilerParams(
            collective_id=1, has_side_effects=True, vmem_limit_bytes=8 * MIB
        ),
        name="relay",
    )(written, held_f, d0, d1, gp, go)

    pcopy, ocopy = pl.pallas_call(
        finish_kernel,
        in_specs=[vm] * 7 + [hbm] * 2,
        out_specs=[hbm] * 2,
        out_shape=(shape(pcopy.shape, bf16), shape(ocopy.shape, bf16)),
        scratch_shapes=[pltpu.VMEM((size, width), bf16), pltpu.VMEM((width, size), bf16), dma(4)],
        input_output_aliases={7: 0, 8: 1},
        compiler_params=pltpu.CompilerParams(vmem_limit_bytes=4 * MIB),
        name="finish",
    )(held_f, d0, d1, lp, lo, fp, fo, pcopy, ocopy)
    return pn, on, pcopy, ocopy, first.reshape(m1.shape), second.reshape(m2.shape)


def over_tokens(left_rows, right_rows, precise):
    return lax.dot_general(
        left_rows,
        right_rows,
        (((0,), (0,)), ((), ())),
        preferred_element_type=jnp.float32,
        precision=precise,
    )


def body(
    saved_inputs,
    proj_cotangent,
    saved_hidden,
    out_cotangent,
    factors,
    w_proj,
    w_out,
    moment_first,
    moment_second,
):
    highest = lax.Precision.HIGHEST
    fs_count = lax.axis_size("fs")
    tp_count = lax.axis_size("tp")
    d_model = factors.shape[1]
    hidden_width = proj_cotangent.shape[1]
    fs_rows = d_model // fs_count
    tp_feats = saved_inputs.shape[1]
    own_rows = lax.dynamic_slice_in_dim(factors, lax.axis_index("fs") * fs_rows, fs_rows, 1).astype(
        jnp.float32
    )
    own_feats = lax.dynamic_slice_in_dim(factors, lax.axis_index("tp") * tp_feats, tp_feats, 1)
    proj_rows = jnp.dot(saved_inputs, own_feats[0], preferred_element_type=jnp.float32)
    out_rows = jnp.dot(out_cotangent, own_feats[1], preferred_element_type=jnp.float32)
    proj_rows, out_rows = lax.psum((proj_rows, out_rows), "tp")
    partial_sums = jnp.stack(
        [
            over_tokens(proj_rows, proj_cotangent.astype(jnp.float32), highest),
            over_tokens(out_rows, saved_hidden.astype(jnp.float32), highest),
        ]
    )
    small_grads = lax.psum(partial_sums, "fs")
    first_next = beta_first * moment_first + (1.0 - beta_first) * small_grads
    second_next = beta_second * moment_second + (1.0 - beta_second) * small_grads * small_grads
    direction = first_next / (jnp.sqrt(second_next) + epsilon)
    update_full = jnp.einsum("kdr,kre->kde", own_rows, direction, precision=highest)
    squares = lax.psum(jnp.sum(update_full * update_full, axis=(1, 2)), ("fs", "tp"))
    norm_scale = lax.rsqrt(squares / (d_model * hidden_width * tp_count) + epsilon)
    stepped = update_full * norm_scale[:, None, None]
    proj_next = w_proj - learn_rate * stepped[0]
    out_next = w_out - learn_rate * stepped[1].T
    proj_copy, out_copy = (
        lax.all_gather(proj_next.astype(jnp.bfloat16), "fs", axis=0, tiled=True),
        lax.all_gather(out_next.astype(jnp.bfloat16), "fs", axis=1, tiled=True),
    )
    return (proj_next, out_next, proj_copy, out_copy, first_next, second_next)


def solution(mesh):
    placed = (
        P("fs", "tp"),
        P("fs", "tp"),
        P("fs", "tp"),
        P("fs", "tp"),
        P(),
        P("fs", "tp"),
        P("tp", "fs"),
        P(None, None, "tp"),
        P(None, None, "tp"),
    )
    planned = fast_body if mesh.shape["fs"] == 4 and mesh.shape["tp"] == 8 else body
    return jax.shard_map(
        planned,
        mesh=mesh,
        in_specs=placed,
        out_specs=(
            P("fs", "tp"),
            P("tp", "fs"),
            P(None, "tp"),
            P("tp", None),
            P(None, None, "tp"),
            P(None, None, "tp"),
        ),
        check_vma=False,
    )
```

```python
import functools

import jax
import jax.numpy as jnp
from jax import lax
from jax.experimental import pallas as pl
from jax.experimental.pallas import tpu as pltpu
from jax.sharding import PartitionSpec as P

beta_first = 0.9
beta_second = 0.95
learn_rate = 0.02
epsilon = 1e-06
weight_rate = 1328.0
code_top = 200.0
chunks = 4
early = 1
late_cuts = (4, 8, 12, 14, 16)
pieces = 16
pad_rows = 8
lead = 1
MIB = 1024 * 1024
MESH = pl.DeviceIdType.MESH


def encode(x, gain, doublings):
    t = x * gain
    for _ in range(doublings):
        t = t * t
    return jnp.where(x < 0, -t, t).astype(jnp.bfloat16)


def decode(code, gain, doublings):
    v = code.astype(jnp.float32)
    size = jnp.exp2(jnp.log2(jnp.abs(v)) * (0.5**doublings)) * (1.0 / gain)
    return jnp.where(v < 0, -size, size)


def largest(x):
    top = jnp.max(jnp.max(jnp.abs(x), axis=0, keepdims=True), axis=1, keepdims=True)
    return jnp.maximum(top, 1e-30)


def two_parts(x, axis):
    high = x.astype(jnp.bfloat16)
    low = (x - high.astype(jnp.float32)).astype(jnp.bfloat16)
    return jnp.concatenate([high, low], axis=axis)


def proj_step(f, d0):
    return jnp.dot(jnp.concatenate([f, f], axis=1), d0[...], preferred_element_type=jnp.float32)


def out_step(f, d1):
    return lax.dot_general(
        d1[...],
        jnp.concatenate([f, f], axis=1),
        (((1,), (1,)), ((), ())),
        preferred_element_type=jnp.float32,
    )


def weight_code(x):
    return jnp.exp2(x * weight_rate).astype(jnp.bfloat16)


def weight_of(code):
    return jnp.log2(code.astype(jnp.float32)) * (1.0 / weight_rate)


def pack(ref, x):
    top = largest(x).astype(jnp.bfloat16)
    ref[: x.shape[0], :] = encode(x, code_top / top.astype(jnp.float32), 4)
    ref[ref.shape[0] - pad_rows :, :] = jnp.broadcast_to(top, (pad_rows, x.shape[1]))


def unpack(ref, n):
    top = ref[ref.shape[0] - pad_rows :, :][0:1, 0:1].astype(jnp.float32)
    return decode(ref[:n, :], code_top / top, 4)


def exchange_kernel(
    tp_count,
    entries,
    si_hbm,
    pc_hbm,
    sh_hbm,
    oc_hbm,
    f_hbm,
    wp_hbm,
    wo_hbm,
    mf_hbm,
    ms_hbm,
    first_ref,
    second_ref,
    d0_ref,
    d1_ref,
    gp_ref,
    go_ref,
    pn_ref,
    on_ref,
    fp_ref,
    fo_ref,
    f_ref,
    si_ref,
    pc_ref,
    sh_ref,
    oc_ref,
    wp_ref,
    wo_ref,
    mf_ref,
    ms_ref,
    cp,
    co,
    rows,
    pair_in,
    half,
    zc,
    zin,
    zall,
    part,
    pair_a,
    pair_b,
    pair_in_a,
    pair_in_b,
    step_a,
    step_b,
    in_a,
    in_b,
    quarters,
    sq,
    sq_in,
    known,
    in_s,
    out_s,
    out_r,
):
    fs = lax.axis_index("fs")
    tp = lax.axis_index("tp")
    core = lax.rem(tp, 2)
    z = tp // 2
    z_count = tp_count // 2
    across_x = fs + 1 - 2 * lax.rem(fs, 2)
    across_y = lax.rem(fs + 2, 4)
    diagonal = 3 - fs
    partner = tp + 1 - 2 * core
    z_peers = [2 * lax.rem(z + o, z_count) + core for o in range(1, z_count)]
    tp_peers = [lax.rem(tp + o, tp_count) for o in range(1, tp_count)]
    to_x, to_y = {"fs": across_x}, {"fs": across_y}

    def send(src, dst, where, s, r):
        copy = pltpu.make_async_remote_copy(
            src_ref=src,
            dst_ref=dst,
            send_sem=out_s.at[s],
            recv_sem=out_r.at[r],
            device_id=where,
            device_id_type=MESH,
        )
        copy.start()
        return copy

    def whole(ref, s, r):
        return pltpu.make_async_remote_copy(
            src_ref=ref,
            dst_ref=ref,
            send_sem=out_s.at[s],
            recv_sem=out_r.at[r],
            device_id={"tp": partner},
            device_id_type=MESH,
        )

    def signal(sem, where):
        pl.semaphore_signal(sem, inc=1, device_id=where, device_id_type=MESH)

    barrier = pltpu.get_barrier_semaphore()

    d_rows, width = cp.shape

    def share(n, start, stop, of=chunks):
        return pl.ds(start * n // of, (stop - start) * n // of)

    spans = ((0, 2), (2, 6), (6, 10), (10, 15))
    pairs = []
    for start, stop in (spans[0], spans[1], (spans[1][1], pieces)):
        a, b = share(d_rows, start, stop, pieces), share(width, start, stop, pieces)
        pairs += [(wp_hbm.at[a, :], wp_ref.at[a, :]), (wo_hbm.at[b, :], wo_ref.at[b, :])]
    pairs += [
        (f_hbm, f_ref),
        (si_hbm, si_ref),
        (oc_hbm, oc_ref),
        (pc_hbm, pc_ref),
        (sh_hbm, sh_ref),
        (mf_hbm, mf_ref),
        (ms_hbm, ms_ref),
    ]
    loads = [pltpu.make_async_copy(a, b, in_s.at[i]) for i, (a, b) in enumerate(pairs)]
    for c in loads[:2]:
        c.start()

    at_x, at_y = lax.rem(fs, 2), fs // 2

    @pl.when(jnp.logical_and(core == lead, at_x == 0))
    def _():
        signal(barrier, to_x)

    @pl.when(jnp.logical_and(core == lead, at_y == 0))
    def _():
        signal(barrier, to_y)

    @pl.when(core == lead)
    def _():
        signal(barrier, {"tp": partner})

    @pl.when(core != lead)
    def _():
        for p in z_peers:
            signal(barrier, {"tp": p})

    for c in loads[2:4]:
        c.start()


    def encode_proj(start, stop):
        a = share(d_rows, start, stop, pieces)
        cp[a, :] = weight_code(wp_ref[a, :])

    def encode_out(start, stop):
        b = share(width, start, stop, pieces)
        co[b, :] = weight_code(wo_ref[b, :])

    def open_proj(start, stop):
        a = share(d_rows, start, stop, pieces)
        send(cp.at[a, :], gp_ref.at[0, a, :], to_x, 0, 0)

    def open_out(start, stop):
        b = share(width, start, stop, pieces)
        send(co.at[b, :], go_ref.at[1, b, :], to_y, 1, 1)

    @pl.when(jnp.logical_and(core == lead, fs > 0))
    def _():
        pl.semaphore_wait(barrier, at_x + at_y)

    @pl.when(jnp.logical_and(core == lead, at_x == 1))
    def _():
        signal(known.at[2], to_x)

    @pl.when(jnp.logical_and(core == lead, at_y == 1))
    def _():
        signal(known.at[3], to_y)

    loads[0].wait()
    encode_proj(*spans[0])
    loads[1].wait()
    encode_out(*spans[0])

    def first_x():
        @pl.when(at_x == 0)
        def _():
            pl.semaphore_wait(known.at[2], 1)

        open_proj(*spans[0])

    def first_y():
        @pl.when(at_y == 0)
        def _():
            pl.semaphore_wait(known.at[3], 1)

        open_out(*spans[0])

    @pl.when(jnp.logical_and(core == lead, at_x >= at_y))
    def _():
        first_x()
        first_y()

    @pl.when(jnp.logical_and(core == lead, at_x < at_y))
    def _():
        first_y()
        first_x()

    for c in loads[4:]:
        c.start()
    for n, (start, stop) in enumerate(spans[1:]):
        if n < 2:
            loads[2 * n + 2].wait()
            loads[2 * n + 3].wait()
        encode_proj(start, stop)
        encode_out(start, stop)

        @pl.when(core == lead)
        def _(start=start, stop=stop):
            open_proj(start, stop)
            open_out(start, stop)


    @pl.when(core == lead)
    def _():
        pl.semaphore_wait(known.at[1], 1)
        signal(known.at[0], to_x)
        signal(known.at[0], to_y)
        pl.semaphore_wait(known.at[0], 2)
        signal(known.at[0], {"tp": partner})

    @pl.when(core != lead)
    def _():
        pl.semaphore_wait(barrier, z_count)
        signal(known.at[1], {"tp": partner})
        for p in z_peers:
            signal(known.at[1], {"tp": p})
        pl.semaphore_wait(known.at[0], 1)
        open_proj(0, spans[-1][1])
        open_out(0, spans[-1][1])

    last = spans[-1][1]
    encode_proj(last, pieces)
    encode_out(last, pieces)

    def more(start, stop):
        a, b = share(d_rows, start, stop, pieces), share(width, start, stop, pieces)
        send(co.at[b, :], go_ref.at[0, b, :], to_x, 0, 2)
        send(cp.at[a, :], gp_ref.at[1, a, :], to_y, 1, 3)

    cuts = (0, 2, 5, 8, 16)
    for c in loads[6:9]:
        c.wait()

    tokens, feats = si_ref.shape
    own = pl.ds(pl.multiple_of(tp * feats, feats), feats)
    rows[0] = jnp.dot(si_ref[...], f_ref[0, own, :], preferred_element_type=jnp.float32)
    rows[1] = jnp.dot(oc_ref[...], f_ref[1, own, :], preferred_element_type=jnp.float32)
    paired = send(rows.at[1 - core], pair_in, {"tp": partner}, 2, 4)
    for c in loads[9:]:
        c.wait()
    rank = f_ref.shape[2]
    grams = [
        lax.dot_general(f_ref[k], f_ref[k], (((0,), (0,)), ((), ())), preferred_element_type=jnp.float32)
        for k in range(2)
    ]
    paired.wait_recv()
    half[...] = rows[core] + pair_in[...]
    piece = tokens // z_count

    def piece_of(i):
        return pl.ds(pl.multiple_of(i * piece, 8), piece)

    @pl.when(core != lead)
    def _():
        pl.semaphore_wait(known.at[1], z_count - 1)
        signal(known.at[4], {"tp": partner})

    @pl.when(core == lead)
    def _():
        pl.semaphore_wait(known.at[4], 1)

    scatter = []
    for i, p in enumerate(z_peers):
        pack(zc.at[i], half[piece_of(lax.rem(z + i + 1, z_count)), :])
        scatter.append(send(zc.at[i], zin.at[i], {"tp": p}, 3, 5 + i))
    total = half[piece_of(z), :]
    for i, c in enumerate(scatter):
        c.wait_recv()
        total = total + unpack(zin.at[i], piece)
    pack(zall.at[core, z], total)
    def hand(at, where, s, r):
        return send(zall.at[core, at], zall.at[core, at], where, s, r)

    gathers = [hand(z, {"tp": p}, 4, 8 + i) for i, p in enumerate(z_peers)]
    hand(z, {"tp": partner}, 5, 11)
    for i, c in enumerate(gathers):
        c.wait_recv()
        hand(lax.rem(z + z_count - 1 - i, z_count), {"tp": partner}, 5, 11)
    passed = whole(zall.at[core], 5, 11)
    passed.wait_recv()
    paired.wait_send()
    whole(zc, 3, 5).wait_send()
    whole(zc, 4, 5).wait_send()
    passed.wait_send()

    for k, right in enumerate((pc_ref, sh_ref)):
        for i in range(z_count):
            rows[k, i * piece : (i + 1) * piece, :] = unpack(zall.at[k, i], piece)
        left = two_parts(rows[k], 1)
        both = lax.dot_general(
            left, right[...], (((0,), (0,)), ((), ())), preferred_element_type=jnp.float32
        )
        both = both[:rank] + both[rank:]
        for j in range(4):
            part[k, j] = both[:, j * width // 4 : (j + 1) * width // 4]

    pack(pair_a, jnp.concatenate([part[0, across_x], part[0, diagonal]], axis=0))
    pack(pair_b, jnp.concatenate([part[1, across_y], part[1, diagonal]], axis=0))
    sums = [
        send(pair_a, pair_in_a, to_x, 3, 12),
        send(pair_b, pair_in_b, to_y, 4, 13),
    ]
    open_proj(last, pieces)
    open_out(last, pieces)
    more(cuts[0], cuts[1])
    sums[0].wait_recv()
    got_a = unpack(pair_in_a, 2 * rank)
    pack(step_a, part[0, across_y] + got_a[rank:])
    sums.append(send(step_a, in_a, to_y, 7, 14))
    sums[1].wait_recv()
    got_b = unpack(pair_in_b, 2 * rank)
    pack(step_b, part[1, across_x] + got_b[rank:])
    sums.append(send(step_b, in_b, to_x, 8, 15))
    more(cuts[1], cuts[2])
    sums[2].wait_recv()
    pack(quarters.at[0, fs], part[0, fs] + got_a[:rank] + unpack(in_a, rank))

    def spread(k, at, where, r):
        return send(quarters.at[k, at], quarters.at[k, at], where, 5 + k, r)

    from_y = spread(0, fs, to_y, 16)
    spread(0, fs, to_x, 18)
    sums[3].wait_recv()
    pack(quarters.at[1, fs], part[1, fs] + got_b[:rank] + unpack(in_b, rank))
    from_x = spread(1, fs, to_x, 17)
    spread(1, fs, to_y, 18)
    more(cuts[2], cuts[3])
    from_y.wait_recv()
    spread(0, across_y, to_x, 18)
    from_x.wait_recv()
    spread(1, across_x, to_y, 18)
    more(cuts[3], cuts[4])
    whole(gp_ref.at[0], 0, 0).wait_recv()
    whole(go_ref.at[1], 1, 1).wait_recv()

    def relay(i):
        a = share(d_rows, i, i + 1)
        send(gp_ref.at[0, a, :], gp_ref.at[2, a, :], to_y, 1, 20 + 2 * i)
        send(go_ref.at[1, :, a], go_ref.at[2, :, a], to_x, 0, 21 + 2 * i)

    for i in range(early):
        relay(i)

    @pl.when(core != lead)
    def _():
        for i in range(early, chunks):
            relay(i)

    whole(quarters.at[0], 5, 18).wait_recv()
    for c in sums:
        c.wait_send()
    whole(quarters.at[0, 0:3], 5, 12).wait_send()
    whole(quarters.at[1, 0:3], 6, 13).wait_send()

    highest = lax.Precision.HIGHEST
    squares = []
    directions = []
    for k in range(2):
        small = jnp.concatenate([unpack(quarters.at[k, j], rank) for j in range(4)], axis=1)
        at = slice(k * rank, (k + 1) * rank)
        first = beta_first * mf_ref[at, :] + (1.0 - beta_first) * small
        second = beta_second * ms_ref[at, :] + (1.0 - beta_second) * small * small
        first_ref[at, :] = first
        second_ref[at, :] = second
        direction = first / (jnp.sqrt(second) + epsilon)
        directions.append(direction)
        seen = jnp.dot(grams[k], direction, preferred_element_type=jnp.float32, precision=highest)
        seen = jnp.sum(seen * direction, axis=0, keepdims=True)
        squares.append(jnp.sum(seen, axis=1, keepdims=True))
    row = lax.broadcasted_iota(jnp.int32, sq.shape, 0)
    sq[...] = jnp.where(row == 0, squares[0], squares[1])
    for i, p in enumerate(tp_peers):
        send(sq, sq_in.at[i], {"tp": p}, 2, 19)
    whole(sq_in, 2, 19).wait_recv()
    total = sq[...]
    for i in range(tp_count - 1):
        total = total + sq_in[i]
    scale = -learn_rate * lax.rsqrt(jnp.maximum(total, 0.0) / entries + epsilon)
    d0_ref[...] = two_parts(directions[0] * scale[0:1, 0:1], 0)
    d1_ref[...] = two_parts(jnp.transpose(directions[1] * scale[1:2, 0:1]), 1)
    whole(sq_in, 2, 19).wait_send()

    size = d_rows // chunks

    def block(slot, owner, proj_code, out_code, start=0, stop=chunks):
        def one(i, _):
            at = pl.ds(pl.multiple_of(i * size, size), size)
            there = pl.ds(pl.multiple_of(owner * d_rows + i * size, size), size)
            u = proj_step(f_ref[0, there, :], d0_ref)
            fp_ref[slot, at, :] = (weight_of(proj_code[at, :]) + u).astype(jnp.bfloat16)
            if slot == 0:
                pn_ref[at, :] = wp_ref[at, :] + u
            u = out_step(f_ref[1, there, :], d1_ref)
            fo_ref[slot, :, at] = (weight_of(out_code[:, at]) + u).astype(jnp.bfloat16)
            if slot == 0:
                on_ref[:, at] = wo_ref[:, at] + u
            return 0

        lax.fori_loop(start, stop, one, 0)

    block(0, fs, cp, co)
    whole(go_ref.at[0], 0, 2).wait_recv()
    block(1, across_x, gp_ref.at[0], go_ref.at[0])
    whole(gp_ref.at[1], 1, 3).wait_recv()
    block(2, across_y, gp_ref.at[1], go_ref.at[1])

    def relayed(i):
        a = share(d_rows, i, i + 1)
        whole(gp_ref.at[2, a, :], 1, 20 + 2 * i).wait_recv()
        whole(go_ref.at[2, :, a], 0, 21 + 2 * i).wait_recv()
        block(3, diagonal, gp_ref.at[2], go_ref.at[2], i, i + 1)

    for i in range(early):
        relayed(i)
    whole(go_ref.at[0:2], 0, 0).wait_send()
    whole(gp_ref.at[0:2], 1, 1).wait_send()
    a = share(d_rows, 0, early)
    whole(gp_ref.at[2, a, :], 1, 0).wait_send()
    whole(go_ref.at[2, :, a], 0, 0).wait_send()

    @pl.when(core != lead)
    def _():
        for i in range(early, chunks):
            relayed(i)
        a = share(d_rows, early, chunks)
        whole(gp_ref.at[2, a, :], 1, 0).wait_send()
        whole(go_ref.at[2, :, a], 0, 0).wait_send()


def write_kernel(
    pn, on, fp, fo, mf, ms,
    pn_hbm, on_hbm, pc_hbm, oc_hbm, first_hbm, second_hbm, written, sems
):
    me = lax.axis_index("fs")
    core = lax.rem(lax.axis_index("tp"), 2)
    d_rows = pn.shape[0]
    size = d_rows // chunks

    def span(owner, start=0, stop=chunks):
        return pl.ds(pl.multiple_of(owner * d_rows + start * size, size), (stop - start) * size)

    def diagonal(start, stop):
        a = pl.ds(start * size, (stop - start) * size)
        there = span(3 - me, start, stop)
        return [(fp.at[3, a, :], pc_hbm.at[there, :]), (fo.at[3, :, a], oc_hbm.at[:, there])]

    pairs = [(pn, pn_hbm), (on, on_hbm), (mf, first_hbm), (ms, second_hbm)]
    for r, owner in enumerate((me, me + 1 - 2 * lax.rem(me, 2), lax.rem(me + 2, 4))):
        pairs += [(fp.at[r], pc_hbm.at[span(owner), :]), (fo.at[r], oc_hbm.at[:, span(owner)])]
    pairs += diagonal(0, early)
    copies = [pltpu.make_async_copy(a, b, sems.at[i]) for i, (a, b) in enumerate(pairs)]
    for c in copies:
        c.start()

    @pl.when(core != lead)
    def _():
        rest = [
            pltpu.make_async_copy(a, b, sems.at[len(copies) + i])
            for i, (a, b) in enumerate(diagonal(early, chunks))
        ]
        for c in rest:
            c.start()
        for c in rest:
            c.wait()

    for c in copies:
        c.wait()
    written[...] = jnp.zeros_like(written)


def relay_kernel(written, f_ref, d0_ref, d1_ref, gp, go, lp_ref, lo_ref, fp_ref, fo_ref, out_s, out_r):
    fs = lax.axis_index("fs")
    core = lax.rem(lax.axis_index("tp"), 2)
    to_x = {"fs": fs + 1 - 2 * lax.rem(fs, 2)}
    to_y = {"fs": lax.rem(fs + 2, 4)}
    d_rows = gp.shape[1]
    first = early * d_rows // chunks

    @pl.when(core == lead)
    def _():
        barrier = pltpu.get_barrier_semaphore()
        for where in (to_x, to_y):
            pl.semaphore_signal(barrier, inc=1, device_id=where, device_id_type=MESH)
        pl.semaphore_wait(barrier, 2)
        copies = []
        for start, stop in zip(late_cuts[:-1], late_cuts[1:]):
            start, stop = start * d_rows // pieces, stop * d_rows // pieces
            a, b = pl.ds(start, stop - start), pl.ds(start - first, stop - start)
            for src, dst, where in (
                (gp.at[0, a, :], lp_ref.at[b, :], to_y),
                (go.at[1, :, a], lo_ref.at[:, b], to_x),
            ):
                c = pltpu.make_async_remote_copy(
                    src_ref=src,
                    dst_ref=dst,
                    send_sem=out_s.at[len(copies) % 2],
                    recv_sem=out_r.at[len(copies)],
                    device_id=where,
                    device_id_type=MESH,
                )
                c.start()
                copies.append(c)
        for i, (start, stop) in enumerate(zip(late_cuts[:-2], late_cuts[1:-1])):
            start, stop = start * d_rows // pieces, stop * d_rows // pieces
            at = slice(start - first, stop - first)
            there = pl.ds(pl.multiple_of((3 - fs) * d_rows + start, d_rows // pieces), stop - start)
            copies[2 * i].wait_recv()
            u = proj_step(f_ref[0, there, :], d0_ref)
            fp_ref[at, :] = (weight_of(lp_ref[at, :]) + u).astype(jnp.bfloat16)
            copies[2 * i + 1].wait_recv()
            u = out_step(f_ref[1, there, :], d1_ref)
            fo_ref[:, at] = (weight_of(lo_ref[:, at]) + u).astype(jnp.bfloat16)
        for c in copies[-2:]:
            c.wait_recv()
        for i, ref in enumerate((lp_ref, lo_ref)):
            pltpu.make_async_remote_copy(
                src_ref=ref,
                dst_ref=ref,
                send_sem=out_s.at[i],
                recv_sem=out_r.at[i],
                device_id=to_x,
                device_id_type=MESH,
            ).wait_send()


def finish_kernel(
    f_ref, d0, d1, lp, lo, fp, fo, pc_in, oc_in, pc_hbm, oc_hbm, last_p, last_o, sems
):
    me = lax.axis_index("fs")
    core = lax.rem(lax.axis_index("tp"), 2)
    d_rows = f_ref.shape[1] // 4
    done, size = fp.shape[0], last_p.shape[0]
    half = fo.shape[0] // 2

    @pl.when(core == lead)
    def _():
        def span(start, n):
            return pl.ds(pl.multiple_of((3 - me) * d_rows + start, size), n)

        there = span(d_rows - size - done, done)
        copies = [
            pltpu.make_async_copy(fp, pc_hbm.at[there, :], sems.at[0]),
            pltpu.make_async_copy(fo.at[:half, :], oc_hbm.at[:half, there], sems.at[1]),
            pltpu.make_async_copy(fo.at[half:, :], oc_hbm.at[half:, there], sems.at[4]),
        ]
        for c in copies:
            c.start()
        there = span(d_rows - size, size)
        u = proj_step(f_ref[0, there, :], d0)
        v = out_step(f_ref[1, there, :], d1)
        last_p[...] = (weight_of(lp[done:, :]) + u).astype(jnp.bfloat16)
        last_o[...] = (weight_of(lo[:, done:]) + v).astype(jnp.bfloat16)
        copies += [
            pltpu.make_async_copy(last_p, pc_hbm.at[there, :], sems.at[2]),
            pltpu.make_async_copy(last_o, oc_hbm.at[:, there], sems.at[3]),
        ]
        for c in copies[3:]:
            c.start()
        for i, c in enumerate(copies):
            c.wait()


def fast_body(si, pc, sh, oc, factors, w_proj, w_out, m1, m2):
    tp_count = lax.axis_size("tp")
    kinds, d_model, rank = factors.shape
    tokens = si.shape[0]
    width = pc.shape[1]
    d_rows = w_proj.shape[0]
    f32, bf16 = jnp.float32, jnp.bfloat16
    mf, ms = m1.reshape(2 * rank, width), m2.reshape(2 * rank, width)
    vm = pl.BlockSpec(memory_space=pltpu.VMEM)
    hbm = pl.BlockSpec(memory_space=pltpu.HBM)
    dma = lambda n: pltpu.SemaphoreType.DMA((n,))
    shape = jax.ShapeDtypeStruct
    peers = tp_count - 1
    z_count = tp_count // 2
    piece = tokens // z_count
    packed = -(-piece // pad_rows) * pad_rows + pad_rows
    quarter = width // 4
    args = (si, pc, sh, oc, factors, w_proj, w_out, mf, ms)
    held = tuple(pltpu.with_memory_space_constraint(a, pltpu.HBM) for a in args)
    first, second, d0, d1, gp, go, pn, on, fp, fo, held_f = pl.pallas_call(
        functools.partial(exchange_kernel, tp_count, float(d_model * width * tp_count)),
        out_shape=(
            pltpu.VMEM((2 * rank, width), f32),
            pltpu.VMEM((2 * rank, width), f32),
            pltpu.VMEM((2 * rank, width), bf16),
            pltpu.VMEM((width, 2 * rank), bf16),
            pltpu.VMEM((3, d_rows, width), bf16),
            pltpu.VMEM((3, width, d_rows), bf16),
            pltpu.VMEM((d_rows, width), f32),
            pltpu.VMEM((width, d_rows), f32),
            pltpu.VMEM((4, d_rows, width), bf16),
            pltpu.VMEM((4, width, d_rows), bf16),
            pltpu.VMEM(factors.shape, bf16),
        ),
        in_specs=[hbm] * 9,
        out_specs=(vm,) * 11,
        scratch_shapes=[pltpu.VMEM(a.shape, a.dtype) for a in args if a is not factors]
        + [
            pltpu.VMEM((d_rows, width), bf16),
            pltpu.VMEM((width, d_rows), bf16),
            pltpu.VMEM((2, tokens, rank), f32),
            pltpu.VMEM((tokens, rank), f32),
            pltpu.VMEM((tokens, rank), f32),
            pltpu.VMEM((z_count - 1, packed, rank), bf16),
            pltpu.VMEM((z_count - 1, packed, rank), bf16),
            pltpu.VMEM((2, z_count, packed, rank), bf16),
            pltpu.VMEM((2, 4, rank, quarter), f32),
            pltpu.VMEM((2 * rank + pad_rows, quarter), bf16),
            pltpu.VMEM((2 * rank + pad_rows, quarter), bf16),
            pltpu.VMEM((2 * rank + pad_rows, quarter), bf16),
            pltpu.VMEM((2 * rank + pad_rows, quarter), bf16),
            pltpu.VMEM((rank + pad_rows, quarter), bf16),
            pltpu.VMEM((rank + pad_rows, quarter), bf16),
            pltpu.VMEM((rank + pad_rows, quarter), bf16),
            pltpu.VMEM((rank + pad_rows, quarter), bf16),
            pltpu.VMEM((2, 4, rank + pad_rows, quarter), bf16),
            pltpu.VMEM((8, 128), f32),
            pltpu.VMEM((peers, 8, 128), f32),
            pltpu.SemaphoreType.REGULAR((5,)),
            dma(13),
            dma(9),
            dma(20 + 2 * chunks),
        ],
        compiler_params=pltpu.CompilerParams(
            collective_id=0, has_side_effects=True, vmem_limit_bytes=42 * MIB
        ),
        name="exchange",
    )(*held)

    pn, on, pcopy, ocopy, first, second, written = pl.pallas_call(
        write_kernel,
        in_specs=[vm] * 6,
        out_specs=[hbm] * 6 + [vm],
        out_shape=(
            shape(w_proj.shape, f32),
            shape(w_out.shape, f32),
            shape((d_model, width), bf16),
            shape((width, d_model), bf16),
            shape((2 * rank, width), f32),
            shape((2 * rank, width), f32),
            pltpu.VMEM((8, 128), f32),
        ),
        scratch_shapes=[dma(14)],
        compiler_params=pltpu.CompilerParams(vmem_limit_bytes=4 * MIB),
        name="write",
    )(pn, on, fp, fo, first, second)

    size = d_rows * (late_cuts[-1] - late_cuts[-2]) // pieces
    rest = d_rows - early * d_rows // chunks
    count = 2 * len(late_cuts) - 2
    lp, lo, fp, fo = pl.pallas_call(
        relay_kernel,
        in_specs=[vm] * 6,
        out_specs=(vm,) * 4,
        out_shape=(
            pltpu.VMEM((rest, width), bf16),
            pltpu.VMEM((width, rest), bf16),
            pltpu.VMEM((rest - size, width), bf16),
            pltpu.VMEM((width, rest - size), bf16),
        ),
        scratch_shapes=[dma(2), dma(count)],
        compiler_params=pltpu.CompilerParams(
            collective_id=1, has_side_effects=True, vmem_limit_bytes=8 * MIB
        ),
        name="relay",
    )(written, held_f, d0, d1, gp, go)

    pcopy, ocopy = pl.pallas_call(
        finish_kernel,
        in_specs=[vm] * 7 + [hbm] * 2,
        out_specs=[hbm] * 2,
        out_shape=(shape(pcopy.shape, bf16), shape(ocopy.shape, bf16)),
        scratch_shapes=[pltpu.VMEM((size, width), bf16), pltpu.VMEM((width, size), bf16), dma(5)],
        input_output_aliases={7: 0, 8: 1},
        compiler_params=pltpu.CompilerParams(vmem_limit_bytes=4 * MIB),
        name="finish",
    )(held_f, d0, d1, lp, lo, fp, fo, pcopy, ocopy)
    return pn, on, pcopy, ocopy, first.reshape(m1.shape), second.reshape(m2.shape)


def over_tokens(left_rows, right_rows, precise):
    return lax.dot_general(
        left_rows,
        right_rows,
        (((0,), (0,)), ((), ())),
        preferred_element_type=jnp.float32,
        precision=precise,
    )


def body(
    saved_inputs,
    proj_cotangent,
    saved_hidden,
    out_cotangent,
    factors,
    w_proj,
    w_out,
    moment_first,
    moment_second,
):
    highest = lax.Precision.HIGHEST
    fs_count = lax.axis_size("fs")
    tp_count = lax.axis_size("tp")
    d_model = factors.shape[1]
    hidden_width = proj_cotangent.shape[1]
    fs_rows = d_model // fs_count
    tp_feats = saved_inputs.shape[1]
    own_rows = lax.dynamic_slice_in_dim(factors, lax.axis_index("fs") * fs_rows, fs_rows, 1).astype(
        jnp.float32
    )
    own_feats = lax.dynamic_slice_in_dim(factors, lax.axis_index("tp") * tp_feats, tp_feats, 1)
    proj_rows = jnp.dot(saved_inputs, own_feats[0], preferred_element_type=jnp.float32)
    out_rows = jnp.dot(out_cotangent, own_feats[1], preferred_element_type=jnp.float32)
    proj_rows, out_rows = lax.psum((proj_rows, out_rows), "tp")
    partial_sums = jnp.stack(
        [
            over_tokens(proj_rows, proj_cotangent.astype(jnp.float32), highest),
            over_tokens(out_rows, saved_hidden.astype(jnp.float32), highest),
        ]
    )
    small_grads = lax.psum(partial_sums, "fs")
    first_next = beta_first * moment_first + (1.0 - beta_first) * small_grads
    second_next = beta_second * moment_second + (1.0 - beta_second) * small_grads * small_grads
    direction = first_next / (jnp.sqrt(second_next) + epsilon)
    update_full = jnp.einsum("kdr,kre->kde", own_rows, direction, precision=highest)
    squares = lax.psum(jnp.sum(update_full * update_full, axis=(1, 2)), ("fs", "tp"))
    norm_scale = lax.rsqrt(squares / (d_model * hidden_width * tp_count) + epsilon)
    stepped = update_full * norm_scale[:, None, None]
    proj_next = w_proj - learn_rate * stepped[0]
    out_next = w_out - learn_rate * stepped[1].T
    proj_copy, out_copy = (
        lax.all_gather(proj_next.astype(jnp.bfloat16), "fs", axis=0, tiled=True),
        lax.all_gather(out_next.astype(jnp.bfloat16), "fs", axis=1, tiled=True),
    )
    return (proj_next, out_next, proj_copy, out_copy, first_next, second_next)


def solution(mesh):
    placed = (
        P("fs", "tp"),
        P("fs", "tp"),
        P("fs", "tp"),
        P("fs", "tp"),
        P(),
        P("fs", "tp"),
        P("tp", "fs"),
        P(None, None, "tp"),
        P(None, None, "tp"),
    )
    planned = fast_body if mesh.shape["fs"] == 4 and mesh.shape["tp"] == 8 else body
    return jax.shard_map(
        planned,
        mesh=mesh,
        in_specs=placed,
        out_specs=(
            P("fs", "tp"),
            P("tp", "fs"),
            P(None, "tp"),
            P("tp", None),
            P(None, None, "tp"),
            P(None, None, "tp"),
        ),
        check_vma=False,
    )
```

```python
import functools

import jax
import jax.numpy as jnp
from jax import lax
from jax.experimental import pallas as pl
from jax.experimental.pallas import tpu as pltpu
from jax.sharding import PartitionSpec as P

beta_first = 0.9
beta_second = 0.95
learn_rate = 0.02
epsilon = 1e-06
weight_rate = 1328.0
code_top = 200.0
chunks = 4
early = 1
late_cuts = (4, 8, 12, 14, 16)
pieces = 16
pad_rows = 8
lead = 1
MIB = 1024 * 1024
MESH = pl.DeviceIdType.MESH


def encode(x, gain, doublings):
    t = x * gain
    for _ in range(doublings):
        t = t * t
    return jnp.where(x < 0, -t, t).astype(jnp.bfloat16)


def decode(code, gain, doublings):
    v = code.astype(jnp.float32)
    size = jnp.exp2(jnp.log2(jnp.abs(v)) * (0.5**doublings)) * (1.0 / gain)
    return jnp.where(v < 0, -size, size)


def largest(x):
    top = jnp.max(jnp.max(jnp.abs(x), axis=0, keepdims=True), axis=1, keepdims=True)
    return jnp.maximum(top, 1e-30)


def two_parts(x, axis):
    high = x.astype(jnp.bfloat16)
    low = (x - high.astype(jnp.float32)).astype(jnp.bfloat16)
    return jnp.concatenate([high, low], axis=axis)


def proj_step(f, d0):
    return jnp.dot(jnp.concatenate([f, f], axis=1), d0[...], preferred_element_type=jnp.float32)


def out_step(f, d1):
    return lax.dot_general(
        d1[...],
        jnp.concatenate([f, f], axis=1),
        (((1,), (1,)), ((), ())),
        preferred_element_type=jnp.float32,
    )


def weight_code(x):
    return jnp.exp2(x * weight_rate).astype(jnp.bfloat16)


def weight_of(code):
    return jnp.log2(code.astype(jnp.float32)) * (1.0 / weight_rate)


def pack(ref, x):
    top = largest(x).astype(jnp.bfloat16)
    ref[: x.shape[0], :] = encode(x, code_top / top.astype(jnp.float32), 4)
    ref[ref.shape[0] - pad_rows :, :] = jnp.broadcast_to(top, (pad_rows, x.shape[1]))


def unpack(ref, n):
    top = ref[ref.shape[0] - pad_rows :, :][0:1, 0:1].astype(jnp.float32)
    return decode(ref[:n, :], code_top / top, 4)


def exchange_kernel(
    tp_count,
    entries,
    si_hbm,
    pc_hbm,
    sh_hbm,
    oc_hbm,
    f_hbm,
    wp_hbm,
    wo_hbm,
    mf_hbm,
    ms_hbm,
    first_ref,
    second_ref,
    d0_ref,
    d1_ref,
    gp_ref,
    go_ref,
    pn_ref,
    on_ref,
    fp_ref,
    fo_ref,
    f_ref,
    si_ref,
    pc_ref,
    sh_ref,
    oc_ref,
    wp_ref,
    wo_ref,
    mf_ref,
    ms_ref,
    cp,
    co,
    rows,
    pair_in,
    half,
    zc,
    zin,
    zall,
    part,
    pair_a,
    pair_b,
    pair_in_a,
    pair_in_b,
    step_a,
    step_b,
    in_a,
    in_b,
    quarters,
    sq,
    sq_in,
    known,
    in_s,
    out_s,
    out_r,
):
    fs = lax.axis_index("fs")
    tp = lax.axis_index("tp")
    core = lax.rem(tp, 2)
    z = tp // 2
    z_count = tp_count // 2
    across_x = fs + 1 - 2 * lax.rem(fs, 2)
    across_y = lax.rem(fs + 2, 4)
    diagonal = 3 - fs
    partner = tp + 1 - 2 * core
    z_peers = [2 * lax.rem(z + o, z_count) + core for o in range(1, z_count)]
    tp_peers = [lax.rem(tp + o, tp_count) for o in range(1, tp_count)]
    to_x, to_y = {"fs": across_x}, {"fs": across_y}

    def send(src, dst, where, s, r):
        copy = pltpu.make_async_remote_copy(
            src_ref=src,
            dst_ref=dst,
            send_sem=out_s.at[s],
            recv_sem=out_r.at[r],
            device_id=where,
            device_id_type=MESH,
        )
        copy.start()
        return copy

    def whole(ref, s, r):
        return pltpu.make_async_remote_copy(
            src_ref=ref,
            dst_ref=ref,
            send_sem=out_s.at[s],
            recv_sem=out_r.at[r],
            device_id={"tp": partner},
            device_id_type=MESH,
        )

    def signal(sem, where):
        pl.semaphore_signal(sem, inc=1, device_id=where, device_id_type=MESH)

    barrier = pltpu.get_barrier_semaphore()

    d_rows, width = cp.shape

    def share(n, start, stop, of=chunks):
        return pl.ds(start * n // of, (stop - start) * n // of)

    spans = ((0, 2), (2, 6), (6, 10), (10, 15))
    pairs = []
    for start, stop in (spans[0], spans[1], (spans[1][1], pieces)):
        a, b = share(d_rows, start, stop, pieces), share(width, start, stop, pieces)
        pairs += [(wp_hbm.at[a, :], wp_ref.at[a, :]), (wo_hbm.at[b, :], wo_ref.at[b, :])]
    pairs += [
        (f_hbm, f_ref),
        (si_hbm, si_ref),
        (oc_hbm, oc_ref),
        (pc_hbm, pc_ref),
        (sh_hbm, sh_ref),
        (mf_hbm, mf_ref),
        (ms_hbm, ms_ref),
    ]
    loads = [pltpu.make_async_copy(a, b, in_s.at[i]) for i, (a, b) in enumerate(pairs)]
    for c in loads[:2]:
        c.start()

    at_x, at_y = lax.rem(fs, 2), fs // 2

    @pl.when(jnp.logical_and(core == lead, at_x == 0))
    def _():
        signal(barrier, to_x)

    @pl.when(jnp.logical_and(core == lead, at_y == 0))
    def _():
        signal(barrier, to_y)

    @pl.when(core == lead)
    def _():
        signal(barrier, {"tp": partner})

    @pl.when(core != lead)
    def _():
        for p in z_peers:
            signal(barrier, {"tp": p})

    for c in loads[2:4]:
        c.start()


    def encode_proj(start, stop):
        a = share(d_rows, start, stop, pieces)
        cp[a, :] = weight_code(wp_ref[a, :])

    def encode_out(start, stop):
        b = share(width, start, stop, pieces)
        co[b, :] = weight_code(wo_ref[b, :])

    def open_proj(start, stop):
        a = share(d_rows, start, stop, pieces)
        send(cp.at[a, :], gp_ref.at[0, a, :], to_x, 0, 0)

    def open_out(start, stop):
        b = share(width, start, stop, pieces)
        send(co.at[b, :], go_ref.at[1, b, :], to_y, 1, 1)

    @pl.when(jnp.logical_and(core == lead, fs > 0))
    def _():
        pl.semaphore_wait(barrier, at_x + at_y)

    @pl.when(jnp.logical_and(core == lead, at_x == 1))
    def _():
        signal(known.at[2], to_x)

    @pl.when(jnp.logical_and(core == lead, at_y == 1))
    def _():
        signal(known.at[3], to_y)

    loads[0].wait()
    encode_proj(*spans[0])
    loads[1].wait()
    encode_out(*spans[0])

    def first_x():
        @pl.when(at_x == 0)
        def _():
            pl.semaphore_wait(known.at[2], 1)

        open_proj(*spans[0])

    def first_y():
        @pl.when(at_y == 0)
        def _():
            pl.semaphore_wait(known.at[3], 1)

        open_out(*spans[0])

    @pl.when(jnp.logical_and(core == lead, at_x >= at_y))
    def _():
        first_x()
        first_y()

    @pl.when(jnp.logical_and(core == lead, at_x < at_y))
    def _():
        first_y()
        first_x()

    for c in loads[4:]:
        c.start()
    for n, (start, stop) in enumerate(spans[1:]):
        if n < 2:
            loads[2 * n + 2].wait()
            loads[2 * n + 3].wait()
        encode_proj(start, stop)
        encode_out(start, stop)

        @pl.when(core == lead)
        def _(start=start, stop=stop):
            open_proj(start, stop)
            open_out(start, stop)


    @pl.when(core == lead)
    def _():
        pl.semaphore_wait(known.at[1], 1)
        signal(known.at[0], to_x)
        signal(known.at[0], to_y)
        pl.semaphore_wait(known.at[0], 2)
        signal(known.at[0], {"tp": partner})

    @pl.when(core != lead)
    def _():
        pl.semaphore_wait(barrier, z_count)
        signal(known.at[1], {"tp": partner})
        for p in z_peers:
            signal(known.at[1], {"tp": p})
        pl.semaphore_wait(known.at[0], 1)
        open_proj(0, spans[-1][1])
        open_out(0, spans[-1][1])

    last = spans[-1][1]
    encode_proj(last, pieces)
    encode_out(last, pieces)

    def more(start, stop):
        a, b = share(d_rows, start, stop, pieces), share(width, start, stop, pieces)
        send(co.at[b, :], go_ref.at[0, b, :], to_x, 0, 2)
        send(cp.at[a, :], gp_ref.at[1, a, :], to_y, 1, 3)

    cuts = (0, 2, 5, 8, 16)
    for c in loads[6:9]:
        c.wait()

    tokens, feats = si_ref.shape
    own = pl.ds(pl.multiple_of(tp * feats, feats), feats)
    rows[0] = jnp.dot(si_ref[...], f_ref[0, own, :], preferred_element_type=jnp.float32)
    rows[1] = jnp.dot(oc_ref[...], f_ref[1, own, :], preferred_element_type=jnp.float32)
    paired = send(rows.at[1 - core], pair_in, {"tp": partner}, 2, 4)
    for c in loads[9:]:
        c.wait()
    rank = f_ref.shape[2]
    grams = [
        lax.dot_general(f_ref[k], f_ref[k], (((0,), (0,)), ((), ())), preferred_element_type=jnp.float32)
        for k in range(2)
    ]
    paired.wait_recv()
    half[...] = rows[core] + pair_in[...]
    piece = tokens // z_count

    def piece_of(i):
        return pl.ds(pl.multiple_of(i * piece, 8), piece)

    @pl.when(core != lead)
    def _():
        pl.semaphore_wait(known.at[1], z_count - 1)
        signal(known.at[4], {"tp": partner})

    @pl.when(core == lead)
    def _():
        pl.semaphore_wait(known.at[4], 1)

    scatter = []
    for i, p in enumerate(z_peers):
        pack(zc.at[i], half[piece_of(lax.rem(z + i + 1, z_count)), :])
        scatter.append(send(zc.at[i], zin.at[i], {"tp": p}, 3, 5 + i))
    total = half[piece_of(z), :]
    for i, c in enumerate(scatter):
        c.wait_recv()
        total = total + unpack(zin.at[i], piece)
    pack(zall.at[core, z], total)
    def hand(at, where, s, r):
        return send(zall.at[core, at], zall.at[core, at], where, s, r)

    gathers = [hand(z, {"tp": p}, 4, 8 + i) for i, p in enumerate(z_peers)]
    hand(z, {"tp": partner}, 5, 11)
    for i, c in enumerate(gathers):
        c.wait_recv()
        hand(lax.rem(z + z_count - 1 - i, z_count), {"tp": partner}, 5, 11)
    passed = whole(zall.at[core], 5, 11)
    passed.wait_recv()
    paired.wait_send()
    whole(zc, 3, 5).wait_send()
    whole(zc, 4, 5).wait_send()
    passed.wait_send()

    for k, right in enumerate((pc_ref, sh_ref)):
        for i in range(z_count):
            rows[k, i * piece : (i + 1) * piece, :] = unpack(zall.at[k, i], piece)
        left = two_parts(rows[k], 1)
        both = lax.dot_general(
            left, right[...], (((0,), (0,)), ((), ())), preferred_element_type=jnp.float32
        )
        both = both[:rank] + both[rank:]
        for j in range(4):
            part[k, j] = both[:, j * width // 4 : (j + 1) * width // 4]

    pack(pair_a, jnp.concatenate([part[0, across_x], part[0, diagonal]], axis=0))
    pack(pair_b, jnp.concatenate([part[1, across_y], part[1, diagonal]], axis=0))
    sums = [
        send(pair_a, pair_in_a, to_x, 3, 12),
        send(pair_b, pair_in_b, to_y, 4, 13),
    ]
    open_proj(last, pieces)
    open_out(last, pieces)
    more(cuts[0], cuts[1])
    sums[0].wait_recv()
    got_a = unpack(pair_in_a, 2 * rank)
    pack(step_a, part[0, across_y] + got_a[rank:])
    sums.append(send(step_a, in_a, to_y, 7, 14))
    sums[1].wait_recv()
    got_b = unpack(pair_in_b, 2 * rank)
    pack(step_b, part[1, across_x] + got_b[rank:])
    sums.append(send(step_b, in_b, to_x, 8, 15))
    more(cuts[1], cuts[2])
    sums[2].wait_recv()
    pack(quarters.at[0, fs], part[0, fs] + got_a[:rank] + unpack(in_a, rank))

    def spread(k, at, where, r):
        return send(quarters.at[k, at], quarters.at[k, at], where, 5 + k, r)

    from_y = spread(0, fs, to_y, 16)
    spread(0, fs, to_x, 18)
    sums[3].wait_recv()
    pack(quarters.at[1, fs], part[1, fs] + got_b[:rank] + unpack(in_b, rank))
    from_x = spread(1, fs, to_x, 17)
    spread(1, fs, to_y, 18)
    more(cuts[2], cuts[3])
    from_y.wait_recv()
    spread(0, across_y, to_x, 18)
    from_x.wait_recv()
    spread(1, across_x, to_y, 18)
    more(cuts[3], cuts[4])
    whole(gp_ref.at[0], 0, 0).wait_recv()
    whole(go_ref.at[1], 1, 1).wait_recv()

    def relay(i):
        a = share(d_rows, i, i + 1)
        send(gp_ref.at[0, a, :], gp_ref.at[2, a, :], to_y, 1, 20 + 2 * i)
        send(go_ref.at[1, :, a], go_ref.at[2, :, a], to_x, 0, 21 + 2 * i)

    for i in range(early):
        relay(i)

    @pl.when(core != lead)
    def _():
        for i in range(early, chunks):
            relay(i)

    whole(quarters.at[0], 5, 18).wait_recv()
    for c in sums:
        c.wait_send()
    whole(quarters.at[0, 0:3], 5, 12).wait_send()
    whole(quarters.at[1, 0:3], 6, 13).wait_send()

    highest = lax.Precision.HIGHEST
    squares = []
    directions = []
    for k in range(2):
        small = jnp.concatenate([unpack(quarters.at[k, j], rank) for j in range(4)], axis=1)
        at = slice(k * rank, (k + 1) * rank)
        first = beta_first * mf_ref[at, :] + (1.0 - beta_first) * small
        second = beta_second * ms_ref[at, :] + (1.0 - beta_second) * small * small
        first_ref[at, :] = first
        second_ref[at, :] = second
        direction = first / (jnp.sqrt(second) + epsilon)
        directions.append(direction)
        seen = jnp.dot(grams[k], direction, preferred_element_type=jnp.float32, precision=highest)
        seen = jnp.sum(seen * direction, axis=0, keepdims=True)
        squares.append(jnp.sum(seen, axis=1, keepdims=True))
    row = lax.broadcasted_iota(jnp.int32, sq.shape, 0)
    sq[...] = jnp.where(row == 0, squares[0], squares[1])
    for i, p in enumerate(tp_peers):
        send(sq, sq_in.at[i], {"tp": p}, 2, 19)
    whole(sq_in, 2, 19).wait_recv()
    total = sq[...]
    for i in range(tp_count - 1):
        total = total + sq_in[i]
    scale = -learn_rate * lax.rsqrt(jnp.maximum(total, 0.0) / entries + epsilon)
    d0_ref[...] = two_parts(directions[0] * scale[0:1, 0:1], 0)
    d1_ref[...] = two_parts(jnp.transpose(directions[1] * scale[1:2, 0:1]), 1)
    whole(sq_in, 2, 19).wait_send()

    size = d_rows // chunks

    def block(slot, owner, proj_code, out_code, start=0, stop=chunks):
        def one(i, _):
            at = pl.ds(pl.multiple_of(i * size, size), size)
            there = pl.ds(pl.multiple_of(owner * d_rows + i * size, size), size)
            u = proj_step(f_ref[0, there, :], d0_ref)
            fp_ref[slot, at, :] = (weight_of(proj_code[at, :]) + u).astype(jnp.bfloat16)
            if slot == 0:
                pn_ref[at, :] = wp_ref[at, :] + u
            u = out_step(f_ref[1, there, :], d1_ref)
            fo_ref[slot, :, at] = (weight_of(out_code[:, at]) + u).astype(jnp.bfloat16)
            if slot == 0:
                on_ref[:, at] = wo_ref[:, at] + u
            return 0

        lax.fori_loop(start, stop, one, 0)

    block(0, fs, cp, co)
    whole(go_ref.at[0], 0, 2).wait_recv()
    block(1, across_x, gp_ref.at[0], go_ref.at[0])
    whole(gp_ref.at[1], 1, 3).wait_recv()
    block(2, across_y, gp_ref.at[1], go_ref.at[1])

    def relayed(i):
        a = share(d_rows, i, i + 1)
        whole(gp_ref.at[2, a, :], 1, 20 + 2 * i).wait_recv()
        whole(go_ref.at[2, :, a], 0, 21 + 2 * i).wait_recv()
        block(3, diagonal, gp_ref.at[2], go_ref.at[2], i, i + 1)

    for i in range(early):
        relayed(i)
    whole(go_ref.at[0:2], 0, 0).wait_send()
    whole(gp_ref.at[0:2], 1, 1).wait_send()
    a = share(d_rows, 0, early)
    whole(gp_ref.at[2, a, :], 1, 0).wait_send()
    whole(go_ref.at[2, :, a], 0, 0).wait_send()

    @pl.when(core != lead)
    def _():
        for i in range(early, chunks):
            relayed(i)
        a = share(d_rows, early, chunks)
        whole(gp_ref.at[2, a, :], 1, 0).wait_send()
        whole(go_ref.at[2, :, a], 0, 0).wait_send()


def write_kernel(
    pn, on, fp, fo, mf, ms,
    pn_hbm, on_hbm, pc_hbm, oc_hbm, first_hbm, second_hbm, written, sems
):
    me = lax.axis_index("fs")
    core = lax.rem(lax.axis_index("tp"), 2)
    d_rows = pn.shape[0]
    size = d_rows // chunks

    def span(owner, start=0, stop=chunks):
        return pl.ds(pl.multiple_of(owner * d_rows + start * size, size), (stop - start) * size)

    def diagonal(start, stop):
        a = pl.ds(start * size, (stop - start) * size)
        there = span(3 - me, start, stop)
        return [(fp.at[3, a, :], pc_hbm.at[there, :]), (fo.at[3, :, a], oc_hbm.at[:, there])]

    pairs = [(pn, pn_hbm), (on, on_hbm), (mf, first_hbm), (ms, second_hbm)]
    for r, owner in enumerate((me, me + 1 - 2 * lax.rem(me, 2), lax.rem(me + 2, 4))):
        pairs += [(fp.at[r], pc_hbm.at[span(owner), :]), (fo.at[r], oc_hbm.at[:, span(owner)])]
    pairs += diagonal(0, early)
    copies = [pltpu.make_async_copy(a, b, sems.at[i]) for i, (a, b) in enumerate(pairs)]
    for c in copies:
        c.start()

    @pl.when(core != lead)
    def _():
        rest = [
            pltpu.make_async_copy(a, b, sems.at[len(copies) + i])
            for i, (a, b) in enumerate(diagonal(early, chunks))
        ]
        for c in rest:
            c.start()
        for c in rest:
            c.wait()

    for c in copies:
        c.wait()
    written[...] = jnp.zeros_like(written)


def relay_kernel(
    written, f_ref, d0_ref, d1_ref, gp, go, lp_ref, lo_ref, fp_ref, fo_ref, up_ref, uo_ref, out_s, out_r
):
    fs = lax.axis_index("fs")
    core = lax.rem(lax.axis_index("tp"), 2)
    to_x = {"fs": fs + 1 - 2 * lax.rem(fs, 2)}
    to_y = {"fs": lax.rem(fs + 2, 4)}
    d_rows = gp.shape[1]
    first = early * d_rows // chunks

    @pl.when(core == lead)
    def _():
        barrier = pltpu.get_barrier_semaphore()
        for where in (to_x, to_y):
            pl.semaphore_signal(barrier, inc=1, device_id=where, device_id_type=MESH)
        pl.semaphore_wait(barrier, 2)
        copies = []
        for start, stop in zip(late_cuts[:-1], late_cuts[1:]):
            start, stop = start * d_rows // pieces, stop * d_rows // pieces
            a, b = pl.ds(start, stop - start), pl.ds(start - first, stop - start)
            for src, dst, where in (
                (gp.at[0, a, :], lp_ref.at[b, :], to_y),
                (go.at[1, :, a], lo_ref.at[:, b], to_x),
            ):
                c = pltpu.make_async_remote_copy(
                    src_ref=src,
                    dst_ref=dst,
                    send_sem=out_s.at[len(copies) % 2],
                    recv_sem=out_r.at[len(copies)],
                    device_id=where,
                    device_id_type=MESH,
                )
                c.start()
                copies.append(c)
        last = d_rows - up_ref.shape[0]
        there = pl.ds(pl.multiple_of((3 - fs) * d_rows + last, up_ref.shape[0]), up_ref.shape[0])
        up_ref[...] = proj_step(f_ref[0, there, :], d0_ref)
        uo_ref[...] = out_step(f_ref[1, there, :], d1_ref)
        for i, (start, stop) in enumerate(zip(late_cuts[:-2], late_cuts[1:-1])):
            start, stop = start * d_rows // pieces, stop * d_rows // pieces
            at = slice(start - first, stop - first)
            there = pl.ds(pl.multiple_of((3 - fs) * d_rows + start, d_rows // pieces), stop - start)
            copies[2 * i].wait_recv()
            u = proj_step(f_ref[0, there, :], d0_ref)
            fp_ref[at, :] = (weight_of(lp_ref[at, :]) + u).astype(jnp.bfloat16)
            copies[2 * i + 1].wait_recv()
            u = out_step(f_ref[1, there, :], d1_ref)
            fo_ref[:, at] = (weight_of(lo_ref[:, at]) + u).astype(jnp.bfloat16)
        for c in copies[-2:]:
            c.wait_recv()
        for i, ref in enumerate((lp_ref, lo_ref)):
            pltpu.make_async_remote_copy(
                src_ref=ref,
                dst_ref=ref,
                send_sem=out_s.at[i],
                recv_sem=out_r.at[i],
                device_id=to_x,
                device_id_type=MESH,
            ).wait_send()


def finish_kernel(lp, lo, fp, fo, up, uo, pc_in, oc_in, pc_hbm, oc_hbm, last_p, last_o, sems):
    me = lax.axis_index("fs")
    core = lax.rem(lax.axis_index("tp"), 2)
    d_rows = pc_hbm.shape[0] // 4
    done, size = fp.shape[0], last_p.shape[0]

    @pl.when(core == lead)
    def _():
        def span(start, n):
            return pl.ds(pl.multiple_of((3 - me) * d_rows + start, size), n)

        there = span(d_rows - size - done, done)
        copies = [
            pltpu.make_async_copy(fp, pc_hbm.at[there, :], sems.at[0]),
            pltpu.make_async_copy(fo, oc_hbm.at[:, there], sems.at[1]),
        ]
        for c in copies:
            c.start()
        there = span(d_rows - size, size)
        last_p[...] = (weight_of(lp[done:, :]) + up[...]).astype(jnp.bfloat16)
        copies.append(pltpu.make_async_copy(last_p, pc_hbm.at[there, :], sems.at[2]))
        copies[-1].start()
        last_o[...] = (weight_of(lo[:, done:]) + uo[...]).astype(jnp.bfloat16)
        copies.append(pltpu.make_async_copy(last_o, oc_hbm.at[:, there], sems.at[3]))
        copies[-1].start()
        for i, c in enumerate(copies):
            c.wait()


def fast_body(si, pc, sh, oc, factors, w_proj, w_out, m1, m2):
    tp_count = lax.axis_size("tp")
    kinds, d_model, rank = factors.shape
    tokens = si.shape[0]
    width = pc.shape[1]
    d_rows = w_proj.shape[0]
    f32, bf16 = jnp.float32, jnp.bfloat16
    mf, ms = m1.reshape(2 * rank, width), m2.reshape(2 * rank, width)
    vm = pl.BlockSpec(memory_space=pltpu.VMEM)
    hbm = pl.BlockSpec(memory_space=pltpu.HBM)
    dma = lambda n: pltpu.SemaphoreType.DMA((n,))
    shape = jax.ShapeDtypeStruct
    peers = tp_count - 1
    z_count = tp_count // 2
    piece = tokens // z_count
    packed = -(-piece // pad_rows) * pad_rows + pad_rows
    quarter = width // 4
    args = (si, pc, sh, oc, factors, w_proj, w_out, mf, ms)
    held = tuple(pltpu.with_memory_space_constraint(a, pltpu.HBM) for a in args)
    first, second, d0, d1, gp, go, pn, on, fp, fo, held_f = pl.pallas_call(
        functools.partial(exchange_kernel, tp_count, float(d_model * width * tp_count)),
        out_shape=(
            pltpu.VMEM((2 * rank, width), f32),
            pltpu.VMEM((2 * rank, width), f32),
            pltpu.VMEM((2 * rank, width), bf16),
            pltpu.VMEM((width, 2 * rank), bf16),
            pltpu.VMEM((3, d_rows, width), bf16),
            pltpu.VMEM((3, width, d_rows), bf16),
            pltpu.VMEM((d_rows, width), f32),
            pltpu.VMEM((width, d_rows), f32),
            pltpu.VMEM((4, d_rows, width), bf16),
            pltpu.VMEM((4, width, d_rows), bf16),
            pltpu.VMEM(factors.shape, bf16),
        ),
        in_specs=[hbm] * 9,
        out_specs=(vm,) * 11,
        scratch_shapes=[pltpu.VMEM(a.shape, a.dtype) for a in args if a is not factors]
        + [
            pltpu.VMEM((d_rows, width), bf16),
            pltpu.VMEM((width, d_rows), bf16),
            pltpu.VMEM((2, tokens, rank), f32),
            pltpu.VMEM((tokens, rank), f32),
            pltpu.VMEM((tokens, rank), f32),
            pltpu.VMEM((z_count - 1, packed, rank), bf16),
            pltpu.VMEM((z_count - 1, packed, rank), bf16),
            pltpu.VMEM((2, z_count, packed, rank), bf16),
            pltpu.VMEM((2, 4, rank, quarter), f32),
            pltpu.VMEM((2 * rank + pad_rows, quarter), bf16),
            pltpu.VMEM((2 * rank + pad_rows, quarter), bf16),
            pltpu.VMEM((2 * rank + pad_rows, quarter), bf16),
            pltpu.VMEM((2 * rank + pad_rows, quarter), bf16),
            pltpu.VMEM((rank + pad_rows, quarter), bf16),
            pltpu.VMEM((rank + pad_rows, quarter), bf16),
            pltpu.VMEM((rank + pad_rows, quarter), bf16),
            pltpu.VMEM((rank + pad_rows, quarter), bf16),
            pltpu.VMEM((2, 4, rank + pad_rows, quarter), bf16),
            pltpu.VMEM((8, 128), f32),
            pltpu.VMEM((peers, 8, 128), f32),
            pltpu.SemaphoreType.REGULAR((5,)),
            dma(13),
            dma(9),
            dma(20 + 2 * chunks),
        ],
        compiler_params=pltpu.CompilerParams(
            collective_id=0, has_side_effects=True, vmem_limit_bytes=42 * MIB
        ),
        name="exchange",
    )(*held)

    pn, on, pcopy, ocopy, first, second, written = pl.pallas_call(
        write_kernel,
        in_specs=[vm] * 6,
        out_specs=[hbm] * 6 + [vm],
        out_shape=(
            shape(w_proj.shape, f32),
            shape(w_out.shape, f32),
            shape((d_model, width), bf16),
            shape((width, d_model), bf16),
            shape((2 * rank, width), f32),
            shape((2 * rank, width), f32),
            pltpu.VMEM((8, 128), f32),
        ),
        scratch_shapes=[dma(14)],
        compiler_params=pltpu.CompilerParams(vmem_limit_bytes=4 * MIB),
        name="write",
    )(pn, on, fp, fo, first, second)

    size = d_rows * (late_cuts[-1] - late_cuts[-2]) // pieces
    rest = d_rows - early * d_rows // chunks
    count = 2 * len(late_cuts) - 2
    lp, lo, fp, fo, up, uo = pl.pallas_call(
        relay_kernel,
        in_specs=[vm] * 6,
        out_specs=(vm,) * 6,
        out_shape=(
            pltpu.VMEM((rest, width), bf16),
            pltpu.VMEM((width, rest), bf16),
            pltpu.VMEM((rest - size, width), bf16),
            pltpu.VMEM((width, rest - size), bf16),
            pltpu.VMEM((size, width), f32),
            pltpu.VMEM((width, size), f32),
        ),
        scratch_shapes=[dma(2), dma(count)],
        compiler_params=pltpu.CompilerParams(
            collective_id=1, has_side_effects=True, vmem_limit_bytes=8 * MIB
        ),
        name="relay",
    )(written, held_f, d0, d1, gp, go)

    pcopy, ocopy = pl.pallas_call(
        finish_kernel,
        in_specs=[vm] * 6 + [hbm] * 2,
        out_specs=[hbm] * 2,
        out_shape=(shape(pcopy.shape, bf16), shape(ocopy.shape, bf16)),
        scratch_shapes=[pltpu.VMEM((size, width), bf16), pltpu.VMEM((width, size), bf16), dma(4)],
        input_output_aliases={6: 0, 7: 1},
        compiler_params=pltpu.CompilerParams(vmem_limit_bytes=4 * MIB),
        name="finish",
    )(lp, lo, fp, fo, up, uo, pcopy, ocopy)
    return pn, on, pcopy, ocopy, first.reshape(m1.shape), second.reshape(m2.shape)


def over_tokens(left_rows, right_rows, precise):
    return lax.dot_general(
        left_rows,
        right_rows,
        (((0,), (0,)), ((), ())),
        preferred_element_type=jnp.float32,
        precision=precise,
    )


def body(
    saved_inputs,
    proj_cotangent,
    saved_hidden,
    out_cotangent,
    factors,
    w_proj,
    w_out,
    moment_first,
    moment_second,
):
    highest = lax.Precision.HIGHEST
    fs_count = lax.axis_size("fs")
    tp_count = lax.axis_size("tp")
    d_model = factors.shape[1]
    hidden_width = proj_cotangent.shape[1]
    fs_rows = d_model // fs_count
    tp_feats = saved_inputs.shape[1]
    own_rows = lax.dynamic_slice_in_dim(factors, lax.axis_index("fs") * fs_rows, fs_rows, 1).astype(
        jnp.float32
    )
    own_feats = lax.dynamic_slice_in_dim(factors, lax.axis_index("tp") * tp_feats, tp_feats, 1)
    proj_rows = jnp.dot(saved_inputs, own_feats[0], preferred_element_type=jnp.float32)
    out_rows = jnp.dot(out_cotangent, own_feats[1], preferred_element_type=jnp.float32)
    proj_rows, out_rows = lax.psum((proj_rows, out_rows), "tp")
    partial_sums = jnp.stack(
        [
            over_tokens(proj_rows, proj_cotangent.astype(jnp.float32), highest),
            over_tokens(out_rows, saved_hidden.astype(jnp.float32), highest),
        ]
    )
    small_grads = lax.psum(partial_sums, "fs")
    first_next = beta_first * moment_first + (1.0 - beta_first) * small_grads
    second_next = beta_second * moment_second + (1.0 - beta_second) * small_grads * small_grads
    direction = first_next / (jnp.sqrt(second_next) + epsilon)
    update_full = jnp.einsum("kdr,kre->kde", own_rows, direction, precision=highest)
    squares = lax.psum(jnp.sum(update_full * update_full, axis=(1, 2)), ("fs", "tp"))
    norm_scale = lax.rsqrt(squares / (d_model * hidden_width * tp_count) + epsilon)
    stepped = update_full * norm_scale[:, None, None]
    proj_next = w_proj - learn_rate * stepped[0]
    out_next = w_out - learn_rate * stepped[1].T
    proj_copy, out_copy = (
        lax.all_gather(proj_next.astype(jnp.bfloat16), "fs", axis=0, tiled=True),
        lax.all_gather(out_next.astype(jnp.bfloat16), "fs", axis=1, tiled=True),
    )
    return (proj_next, out_next, proj_copy, out_copy, first_next, second_next)


def solution(mesh):
    placed = (
        P("fs", "tp"),
        P("fs", "tp"),
        P("fs", "tp"),
        P("fs", "tp"),
        P(),
        P("fs", "tp"),
        P("tp", "fs"),
        P(None, None, "tp"),
        P(None, None, "tp"),
    )
    planned = fast_body if mesh.shape["fs"] == 4 and mesh.shape["tp"] == 8 else body
    return jax.shard_map(
        planned,
        mesh=mesh,
        in_specs=placed,
        out_specs=(
            P("fs", "tp"),
            P("tp", "fs"),
            P(None, "tp"),
            P("tp", None),
            P(None, None, "tp"),
            P(None, None, "tp"),
        ),
        check_vma=False,
    )
```

```python
import functools

import jax
import jax.numpy as jnp
from jax import lax
from jax.experimental import pallas as pl
from jax.experimental.pallas import tpu as pltpu
from jax.sharding import PartitionSpec as P

beta_first = 0.9
beta_second = 0.95
learn_rate = 0.02
epsilon = 1e-06
weight_rate = 1328.0
code_top = 200.0
chunks = 4
early = 1
late_cuts = (4, 8, 12, 14, 16)
pieces = 16
pad_rows = 8
lead = 1
MIB = 1024 * 1024
MESH = pl.DeviceIdType.MESH


def encode(x, gain, doublings):
    t = x * gain
    for _ in range(doublings):
        t = t * t
    return jnp.where(x < 0, -t, t).astype(jnp.bfloat16)


def decode(code, gain, doublings):
    v = code.astype(jnp.float32)
    size = jnp.exp2(jnp.log2(jnp.abs(v)) * (0.5**doublings)) * (1.0 / gain)
    return jnp.where(v < 0, -size, size)


def largest(x):
    top = jnp.max(jnp.max(jnp.abs(x), axis=0, keepdims=True), axis=1, keepdims=True)
    return jnp.maximum(top, 1e-30)


def two_parts(x, axis):
    high = x.astype(jnp.bfloat16)
    low = (x - high.astype(jnp.float32)).astype(jnp.bfloat16)
    return jnp.concatenate([high, low], axis=axis)


def proj_step(f, d0):
    return jnp.dot(jnp.concatenate([f, f], axis=1), d0[...], preferred_element_type=jnp.float32)


def out_step(f, d1):
    return lax.dot_general(
        d1[...],
        jnp.concatenate([f, f], axis=1),
        (((1,), (1,)), ((), ())),
        preferred_element_type=jnp.float32,
    )


def weight_code(x):
    return jnp.exp2(x * weight_rate).astype(jnp.bfloat16)


def weight_of(code):
    return jnp.log2(code.astype(jnp.float32)) * (1.0 / weight_rate)


def pack(ref, x):
    top = largest(x).astype(jnp.bfloat16)
    ref[: x.shape[0], :] = encode(x, code_top / top.astype(jnp.float32), 4)
    ref[ref.shape[0] - pad_rows :, :] = jnp.broadcast_to(top, (pad_rows, x.shape[1]))


def unpack(ref, n):
    top = ref[ref.shape[0] - pad_rows :, :][0:1, 0:1].astype(jnp.float32)
    return decode(ref[:n, :], code_top / top, 4)


def exchange_kernel(
    tp_count,
    entries,
    si_hbm,
    pc_hbm,
    sh_hbm,
    oc_hbm,
    f_hbm,
    wp_hbm,
    wo_hbm,
    mf_hbm,
    ms_hbm,
    first_ref,
    second_ref,
    d0_ref,
    d1_ref,
    gp_ref,
    go_ref,
    pn_ref,
    on_ref,
    fp_ref,
    fo_ref,
    f_ref,
    si_ref,
    pc_ref,
    sh_ref,
    oc_ref,
    wp_ref,
    wo_ref,
    mf_ref,
    ms_ref,
    cp,
    co,
    rows,
    pair_in,
    half,
    zc,
    zin,
    zall,
    part,
    pair_a,
    pair_b,
    pair_in_a,
    pair_in_b,
    step_a,
    step_b,
    in_a,
    in_b,
    quarters,
    sq,
    sq_in,
    known,
    in_s,
    out_s,
    out_r,
):
    fs = lax.axis_index("fs")
    tp = lax.axis_index("tp")
    core = lax.rem(tp, 2)
    z = tp // 2
    z_count = tp_count // 2
    across_x = fs + 1 - 2 * lax.rem(fs, 2)
    across_y = lax.rem(fs + 2, 4)
    diagonal = 3 - fs
    partner = tp + 1 - 2 * core
    z_peers = [2 * lax.rem(z + o, z_count) + core for o in range(1, z_count)]
    tp_peers = [lax.rem(tp + o, tp_count) for o in range(1, tp_count)]
    to_x, to_y = {"fs": across_x}, {"fs": across_y}

    def send(src, dst, where, s, r):
        copy = pltpu.make_async_remote_copy(
            src_ref=src,
            dst_ref=dst,
            send_sem=out_s.at[s],
            recv_sem=out_r.at[r],
            device_id=where,
            device_id_type=MESH,
        )
        copy.start()
        return copy

    def whole(ref, s, r):
        return pltpu.make_async_remote_copy(
            src_ref=ref,
            dst_ref=ref,
            send_sem=out_s.at[s],
            recv_sem=out_r.at[r],
            device_id={"tp": partner},
            device_id_type=MESH,
        )

    def signal(sem, where):
        pl.semaphore_signal(sem, inc=1, device_id=where, device_id_type=MESH)

    barrier = pltpu.get_barrier_semaphore()

    d_rows, width = cp.shape

    def share(n, start, stop, of=chunks):
        return pl.ds(start * n // of, (stop - start) * n // of)

    spans = ((0, 2), (2, 6), (6, 10), (10, 15))
    pairs = []
    for start, stop in (spans[0], spans[1], (spans[1][1], pieces)):
        a, b = share(d_rows, start, stop, pieces), share(width, start, stop, pieces)
        pairs += [(wp_hbm.at[a, :], wp_ref.at[a, :]), (wo_hbm.at[b, :], wo_ref.at[b, :])]
    pairs += [
        (f_hbm, f_ref),
        (si_hbm, si_ref),
        (oc_hbm, oc_ref),
        (pc_hbm, pc_ref),
        (sh_hbm, sh_ref),
        (mf_hbm, mf_ref),
        (ms_hbm, ms_ref),
    ]
    loads = [pltpu.make_async_copy(a, b, in_s.at[i]) for i, (a, b) in enumerate(pairs)]
    for c in loads[:2]:
        c.start()

    at_x, at_y = lax.rem(fs, 2), fs // 2

    @pl.when(jnp.logical_and(core == lead, at_x == 0))
    def _():
        signal(barrier, to_x)

    @pl.when(jnp.logical_and(core == lead, at_y == 0))
    def _():
        signal(barrier, to_y)

    @pl.when(core == lead)
    def _():
        signal(barrier, {"tp": partner})

    @pl.when(core != lead)
    def _():
        for p in z_peers:
            signal(barrier, {"tp": p})

    for c in loads[2:4]:
        c.start()


    def encode_proj(start, stop):
        a = share(d_rows, start, stop, pieces)
        cp[a, :] = weight_code(wp_ref[a, :])

    def encode_out(start, stop):
        b = share(width, start, stop, pieces)
        co[b, :] = weight_code(wo_ref[b, :])

    def open_proj(start, stop):
        a = share(d_rows, start, stop, pieces)
        send(cp.at[a, :], gp_ref.at[0, a, :], to_x, 0, 0)

    def open_out(start, stop):
        b = share(width, start, stop, pieces)
        send(co.at[b, :], go_ref.at[1, b, :], to_y, 1, 1)

    @pl.when(jnp.logical_and(core == lead, fs > 0))
    def _():
        pl.semaphore_wait(barrier, at_x + at_y)

    @pl.when(jnp.logical_and(core == lead, at_x == 1))
    def _():
        signal(known.at[2], to_x)

    @pl.when(jnp.logical_and(core == lead, at_y == 1))
    def _():
        signal(known.at[3], to_y)


    def first_x():
        loads[0].wait()
        encode_proj(*spans[0])

        @pl.when(at_x == 0)
        def _():
            pl.semaphore_wait(known.at[2], 1)

        open_proj(*spans[0])

    def first_y():
        loads[1].wait()
        encode_out(*spans[0])

        @pl.when(at_y == 0)
        def _():
            pl.semaphore_wait(known.at[3], 1)

        open_out(*spans[0])

    @pl.when(core != lead)
    def _():
        loads[0].wait()
        encode_proj(*spans[0])
        loads[1].wait()
        encode_out(*spans[0])

    @pl.when(jnp.logical_and(core == lead, at_x >= at_y))
    def _():
        first_x()
        first_y()

    @pl.when(jnp.logical_and(core == lead, at_x < at_y))
    def _():
        first_y()
        first_x()

    for c in loads[4:]:
        c.start()
    for n, (start, stop) in enumerate(spans[1:]):
        if n < 2:
            loads[2 * n + 2].wait()
            loads[2 * n + 3].wait()
        encode_proj(start, stop)
        encode_out(start, stop)

        @pl.when(core == lead)
        def _(start=start, stop=stop):
            open_proj(start, stop)
            open_out(start, stop)


    @pl.when(core == lead)
    def _():
        pl.semaphore_wait(known.at[1], 1)
        signal(known.at[0], to_x)
        signal(known.at[0], to_y)
        pl.semaphore_wait(known.at[0], 2)
        signal(known.at[0], {"tp": partner})

    @pl.when(core != lead)
    def _():
        pl.semaphore_wait(barrier, z_count)
        signal(known.at[1], {"tp": partner})
        for p in z_peers:
            signal(known.at[1], {"tp": p})
        pl.semaphore_wait(known.at[0], 1)
        open_proj(0, spans[-1][1])
        open_out(0, spans[-1][1])

    last = spans[-1][1]
    encode_proj(last, pieces)
    encode_out(last, pieces)

    def more(start, stop):
        a, b = share(d_rows, start, stop, pieces), share(width, start, stop, pieces)
        send(co.at[b, :], go_ref.at[0, b, :], to_x, 0, 2)
        send(cp.at[a, :], gp_ref.at[1, a, :], to_y, 1, 3)

    cuts = (0, 2, 5, 8, 16)
    for c in loads[6:9]:
        c.wait()

    tokens, feats = si_ref.shape
    own = pl.ds(pl.multiple_of(tp * feats, feats), feats)
    rows[0] = jnp.dot(si_ref[...], f_ref[0, own, :], preferred_element_type=jnp.float32)
    rows[1] = jnp.dot(oc_ref[...], f_ref[1, own, :], preferred_element_type=jnp.float32)
    paired = send(rows.at[1 - core], pair_in, {"tp": partner}, 2, 4)
    for c in loads[9:]:
        c.wait()
    rank = f_ref.shape[2]
    grams = [
        lax.dot_general(f_ref[k], f_ref[k], (((0,), (0,)), ((), ())), preferred_element_type=jnp.float32)
        for k in range(2)
    ]
    paired.wait_recv()
    half[...] = rows[core] + pair_in[...]
    piece = tokens // z_count

    def piece_of(i):
        return pl.ds(pl.multiple_of(i * piece, 8), piece)

    @pl.when(core != lead)
    def _():
        pl.semaphore_wait(known.at[1], z_count - 1)
        signal(known.at[4], {"tp": partner})

    @pl.when(core == lead)
    def _():
        pl.semaphore_wait(known.at[4], 1)

    scatter = []
    for i, p in enumerate(z_peers):
        pack(zc.at[i], half[piece_of(lax.rem(z + i + 1, z_count)), :])
        scatter.append(send(zc.at[i], zin.at[i], {"tp": p}, 3, 5 + i))
    total = half[piece_of(z), :]
    for i, c in enumerate(scatter):
        c.wait_recv()
        total = total + unpack(zin.at[i], piece)
    pack(zall.at[core, z], total)
    def hand(at, where, s, r):
        return send(zall.at[core, at], zall.at[core, at], where, s, r)

    gathers = [hand(z, {"tp": p}, 4, 8 + i) for i, p in enumerate(z_peers)]
    hand(z, {"tp": partner}, 5, 11)
    for i, c in enumerate(gathers):
        c.wait_recv()
        hand(lax.rem(z + z_count - 1 - i, z_count), {"tp": partner}, 5, 11)
    passed = whole(zall.at[core], 5, 11)
    passed.wait_recv()
    paired.wait_send()
    whole(zc, 3, 5).wait_send()
    whole(zc, 4, 5).wait_send()
    passed.wait_send()

    for k, right in enumerate((pc_ref, sh_ref)):
        for i in range(z_count):
            rows[k, i * piece : (i + 1) * piece, :] = unpack(zall.at[k, i], piece)
        left = two_parts(rows[k], 1)
        both = lax.dot_general(
            left, right[...], (((0,), (0,)), ((), ())), preferred_element_type=jnp.float32
        )
        both = both[:rank] + both[rank:]
        for j in range(4):
            part[k, j] = both[:, j * width // 4 : (j + 1) * width // 4]

    pack(pair_a, jnp.concatenate([part[0, across_x], part[0, diagonal]], axis=0))
    pack(pair_b, jnp.concatenate([part[1, across_y], part[1, diagonal]], axis=0))
    sums = [
        send(pair_a, pair_in_a, to_x, 3, 12),
        send(pair_b, pair_in_b, to_y, 4, 13),
    ]
    open_proj(last, pieces)
    open_out(last, pieces)
    more(cuts[0], cuts[1])
    sums[0].wait_recv()
    got_a = unpack(pair_in_a, 2 * rank)
    pack(step_a, part[0, across_y] + got_a[rank:])
    sums.append(send(step_a, in_a, to_y, 7, 14))
    sums[1].wait_recv()
    got_b = unpack(pair_in_b, 2 * rank)
    pack(step_b, part[1, across_x] + got_b[rank:])
    sums.append(send(step_b, in_b, to_x, 8, 15))
    more(cuts[1], cuts[2])
    sums[2].wait_recv()
    pack(quarters.at[0, fs], part[0, fs] + got_a[:rank] + unpack(in_a, rank))

    def spread(k, at, where, r):
        return send(quarters.at[k, at], quarters.at[k, at], where, 5 + k, r)

    from_y = spread(0, fs, to_y, 16)
    spread(0, fs, to_x, 18)
    sums[3].wait_recv()
    pack(quarters.at[1, fs], part[1, fs] + got_b[:rank] + unpack(in_b, rank))
    from_x = spread(1, fs, to_x, 17)
    spread(1, fs, to_y, 18)
    more(cuts[2], cuts[3])
    from_y.wait_recv()
    spread(0, across_y, to_x, 18)
    from_x.wait_recv()
    spread(1, across_x, to_y, 18)
    more(cuts[3], cuts[4])
    whole(gp_ref.at[0], 0, 0).wait_recv()
    whole(go_ref.at[1], 1, 1).wait_recv()

    def relay(i):
        a = share(d_rows, i, i + 1)
        send(gp_ref.at[0, a, :], gp_ref.at[2, a, :], to_y, 1, 20 + 2 * i)
        send(go_ref.at[1, :, a], go_ref.at[2, :, a], to_x, 0, 21 + 2 * i)

    for i in range(early):
        relay(i)

    @pl.when(core != lead)
    def _():
        for i in range(early, chunks):
            relay(i)

    whole(quarters.at[0], 5, 18).wait_recv()
    for c in sums:
        c.wait_send()
    whole(quarters.at[0, 0:3], 5, 12).wait_send()
    whole(quarters.at[1, 0:3], 6, 13).wait_send()

    highest = lax.Precision.HIGHEST
    squares = []
    directions = []
    for k in range(2):
        small = jnp.concatenate([unpack(quarters.at[k, j], rank) for j in range(4)], axis=1)
        at = slice(k * rank, (k + 1) * rank)
        first = beta_first * mf_ref[at, :] + (1.0 - beta_first) * small
        second = beta_second * ms_ref[at, :] + (1.0 - beta_second) * small * small
        first_ref[at, :] = first
        second_ref[at, :] = second
        direction = first / (jnp.sqrt(second) + epsilon)
        directions.append(direction)
        seen = jnp.dot(grams[k], direction, preferred_element_type=jnp.float32, precision=highest)
        seen = jnp.sum(seen * direction, axis=0, keepdims=True)
        squares.append(jnp.sum(seen, axis=1, keepdims=True))
    row = lax.broadcasted_iota(jnp.int32, sq.shape, 0)
    sq[...] = jnp.where(row == 0, squares[0], squares[1])
    for i, p in enumerate(tp_peers):
        send(sq, sq_in.at[i], {"tp": p}, 2, 19)
    whole(sq_in, 2, 19).wait_recv()
    total = sq[...]
    for i in range(tp_count - 1):
        total = total + sq_in[i]
    scale = -learn_rate * lax.rsqrt(jnp.maximum(total, 0.0) / entries + epsilon)
    d0_ref[...] = two_parts(directions[0] * scale[0:1, 0:1], 0)
    d1_ref[...] = two_parts(jnp.transpose(directions[1] * scale[1:2, 0:1]), 1)
    whole(sq_in, 2, 19).wait_send()

    size = d_rows // chunks

    def block(slot, owner, proj_code, out_code, start=0, stop=chunks):
        def one(i, _):
            at = pl.ds(pl.multiple_of(i * size, size), size)
            there = pl.ds(pl.multiple_of(owner * d_rows + i * size, size), size)
            u = proj_step(f_ref[0, there, :], d0_ref)
            fp_ref[slot, at, :] = (weight_of(proj_code[at, :]) + u).astype(jnp.bfloat16)
            if slot == 0:
                pn_ref[at, :] = wp_ref[at, :] + u
            u = out_step(f_ref[1, there, :], d1_ref)
            fo_ref[slot, :, at] = (weight_of(out_code[:, at]) + u).astype(jnp.bfloat16)
            if slot == 0:
                on_ref[:, at] = wo_ref[:, at] + u
            return 0

        lax.fori_loop(start, stop, one, 0)

    block(0, fs, cp, co)
    whole(go_ref.at[0], 0, 2).wait_recv()
    block(1, across_x, gp_ref.at[0], go_ref.at[0])
    whole(gp_ref.at[1], 1, 3).wait_recv()
    block(2, across_y, gp_ref.at[1], go_ref.at[1])

    def relayed(i):
        a = share(d_rows, i, i + 1)
        whole(gp_ref.at[2, a, :], 1, 20 + 2 * i).wait_recv()
        whole(go_ref.at[2, :, a], 0, 21 + 2 * i).wait_recv()
        block(3, diagonal, gp_ref.at[2], go_ref.at[2], i, i + 1)

    for i in range(early):
        relayed(i)
    whole(go_ref.at[0:2], 0, 0).wait_send()
    whole(gp_ref.at[0:2], 1, 1).wait_send()
    a = share(d_rows, 0, early)
    whole(gp_ref.at[2, a, :], 1, 0).wait_send()
    whole(go_ref.at[2, :, a], 0, 0).wait_send()

    @pl.when(core != lead)
    def _():
        for i in range(early, chunks):
            relayed(i)
        a = share(d_rows, early, chunks)
        whole(gp_ref.at[2, a, :], 1, 0).wait_send()
        whole(go_ref.at[2, :, a], 0, 0).wait_send()


def write_kernel(
    pn, on, fp, fo, mf, ms,
    pn_hbm, on_hbm, pc_hbm, oc_hbm, first_hbm, second_hbm, written, sems
):
    me = lax.axis_index("fs")
    core = lax.rem(lax.axis_index("tp"), 2)
    d_rows = pn.shape[0]
    size = d_rows // chunks

    def span(owner, start=0, stop=chunks):
        return pl.ds(pl.multiple_of(owner * d_rows + start * size, size), (stop - start) * size)

    def diagonal(start, stop):
        a = pl.ds(start * size, (stop - start) * size)
        there = span(3 - me, start, stop)
        return [(fp.at[3, a, :], pc_hbm.at[there, :]), (fo.at[3, :, a], oc_hbm.at[:, there])]

    pairs = [(pn, pn_hbm), (on, on_hbm), (mf, first_hbm), (ms, second_hbm)]
    for r, owner in enumerate((me, me + 1 - 2 * lax.rem(me, 2), lax.rem(me + 2, 4))):
        pairs += [(fp.at[r], pc_hbm.at[span(owner), :]), (fo.at[r], oc_hbm.at[:, span(owner)])]
    pairs += diagonal(0, early)
    copies = [pltpu.make_async_copy(a, b, sems.at[i]) for i, (a, b) in enumerate(pairs)]
    for c in copies:
        c.start()

    @pl.when(core != lead)
    def _():
        rest = [
            pltpu.make_async_copy(a, b, sems.at[len(copies) + i])
            for i, (a, b) in enumerate(diagonal(early, chunks))
        ]
        for c in rest:
            c.start()
        for c in rest:
            c.wait()

    for c in copies:
        c.wait()
    written[...] = jnp.zeros_like(written)


def relay_kernel(
    written, f_ref, d0_ref, d1_ref, gp, go, lp_ref, lo_ref, fp_ref, fo_ref, up_ref, uo_ref, out_s, out_r
):
    fs = lax.axis_index("fs")
    core = lax.rem(lax.axis_index("tp"), 2)
    to_x = {"fs": fs + 1 - 2 * lax.rem(fs, 2)}
    to_y = {"fs": lax.rem(fs + 2, 4)}
    d_rows = gp.shape[1]
    first = early * d_rows // chunks

    @pl.when(core == lead)
    def _():
        barrier = pltpu.get_barrier_semaphore()
        for where in (to_x, to_y):
            pl.semaphore_signal(barrier, inc=1, device_id=where, device_id_type=MESH)
        pl.semaphore_wait(barrier, 2)
        copies = []
        for start, stop in zip(late_cuts[:-1], late_cuts[1:]):
            start, stop = start * d_rows // pieces, stop * d_rows // pieces
            a, b = pl.ds(start, stop - start), pl.ds(start - first, stop - start)
            for src, dst, where in (
                (gp.at[0, a, :], lp_ref.at[b, :], to_y),
                (go.at[1, :, a], lo_ref.at[:, b], to_x),
            ):
                c = pltpu.make_async_remote_copy(
                    src_ref=src,
                    dst_ref=dst,
                    send_sem=out_s.at[len(copies) % 2],
                    recv_sem=out_r.at[len(copies)],
                    device_id=where,
                    device_id_type=MESH,
                )
                c.start()
                copies.append(c)
        last = d_rows - up_ref.shape[0]
        there = pl.ds(pl.multiple_of((3 - fs) * d_rows + last, up_ref.shape[0]), up_ref.shape[0])
        up_ref[...] = proj_step(f_ref[0, there, :], d0_ref)
        uo_ref[...] = out_step(f_ref[1, there, :], d1_ref)
        for i, (start, stop) in enumerate(zip(late_cuts[:-2], late_cuts[1:-1])):
            start, stop = start * d_rows // pieces, stop * d_rows // pieces
            at = slice(start - first, stop - first)
            there = pl.ds(pl.multiple_of((3 - fs) * d_rows + start, d_rows // pieces), stop - start)
            copies[2 * i].wait_recv()
            u = proj_step(f_ref[0, there, :], d0_ref)
            fp_ref[at, :] = (weight_of(lp_ref[at, :]) + u).astype(jnp.bfloat16)
            copies[2 * i + 1].wait_recv()
            u = out_step(f_ref[1, there, :], d1_ref)
            fo_ref[:, at] = (weight_of(lo_ref[:, at]) + u).astype(jnp.bfloat16)
        for c in copies[-2:]:
            c.wait_recv()
        for i, ref in enumerate((lp_ref, lo_ref)):
            pltpu.make_async_remote_copy(
                src_ref=ref,
                dst_ref=ref,
                send_sem=out_s.at[i],
                recv_sem=out_r.at[i],
                device_id=to_x,
                device_id_type=MESH,
            ).wait_send()


def finish_kernel(lp, lo, fp, fo, up, uo, pc_in, oc_in, pc_hbm, oc_hbm, last_p, last_o, sems):
    me = lax.axis_index("fs")
    core = lax.rem(lax.axis_index("tp"), 2)
    d_rows = pc_hbm.shape[0] // 4
    done, size = fp.shape[0], last_p.shape[0]

    @pl.when(core == lead)
    def _():
        def span(start, n):
            return pl.ds(pl.multiple_of((3 - me) * d_rows + start, size), n)

        there = span(d_rows - size - done, done)
        copies = [
            pltpu.make_async_copy(fp, pc_hbm.at[there, :], sems.at[0]),
            pltpu.make_async_copy(fo, oc_hbm.at[:, there], sems.at[1]),
        ]
        for c in copies:
            c.start()
        there = span(d_rows - size, size)
        last_p[...] = (weight_of(lp[done:, :]) + up[...]).astype(jnp.bfloat16)
        copies.append(pltpu.make_async_copy(last_p, pc_hbm.at[there, :], sems.at[2]))
        copies[-1].start()
        last_o[...] = (weight_of(lo[:, done:]) + uo[...]).astype(jnp.bfloat16)
        copies.append(pltpu.make_async_copy(last_o, oc_hbm.at[:, there], sems.at[3]))
        copies[-1].start()
        for i, c in enumerate(copies):
            c.wait()


def fast_body(si, pc, sh, oc, factors, w_proj, w_out, m1, m2):
    tp_count = lax.axis_size("tp")
    kinds, d_model, rank = factors.shape
    tokens = si.shape[0]
    width = pc.shape[1]
    d_rows = w_proj.shape[0]
    f32, bf16 = jnp.float32, jnp.bfloat16
    mf, ms = m1.reshape(2 * rank, width), m2.reshape(2 * rank, width)
    vm = pl.BlockSpec(memory_space=pltpu.VMEM)
    hbm = pl.BlockSpec(memory_space=pltpu.HBM)
    dma = lambda n: pltpu.SemaphoreType.DMA((n,))
    shape = jax.ShapeDtypeStruct
    peers = tp_count - 1
    z_count = tp_count // 2
    piece = tokens // z_count
    packed = -(-piece // pad_rows) * pad_rows + pad_rows
    quarter = width // 4
    args = (si, pc, sh, oc, factors, w_proj, w_out, mf, ms)
    held = tuple(pltpu.with_memory_space_constraint(a, pltpu.HBM) for a in args)
    first, second, d0, d1, gp, go, pn, on, fp, fo, held_f = pl.pallas_call(
        functools.partial(exchange_kernel, tp_count, float(d_model * width * tp_count)),
        out_shape=(
            pltpu.VMEM((2 * rank, width), f32),
            pltpu.VMEM((2 * rank, width), f32),
            pltpu.VMEM((2 * rank, width), bf16),
            pltpu.VMEM((width, 2 * rank), bf16),
            pltpu.VMEM((3, d_rows, width), bf16),
            pltpu.VMEM((3, width, d_rows), bf16),
            pltpu.VMEM((d_rows, width), f32),
            pltpu.VMEM((width, d_rows), f32),
            pltpu.VMEM((4, d_rows, width), bf16),
            pltpu.VMEM((4, width, d_rows), bf16),
            pltpu.VMEM(factors.shape, bf16),
        ),
        in_specs=[hbm] * 9,
        out_specs=(vm,) * 11,
        scratch_shapes=[pltpu.VMEM(a.shape, a.dtype) for a in args if a is not factors]
        + [
            pltpu.VMEM((d_rows, width), bf16),
            pltpu.VMEM((width, d_rows), bf16),
            pltpu.VMEM((2, tokens, rank), f32),
            pltpu.VMEM((tokens, rank), f32),
            pltpu.VMEM((tokens, rank), f32),
            pltpu.VMEM((z_count - 1, packed, rank), bf16),
            pltpu.VMEM((z_count - 1, packed, rank), bf16),
            pltpu.VMEM((2, z_count, packed, rank), bf16),
            pltpu.VMEM((2, 4, rank, quarter), f32),
            pltpu.VMEM((2 * rank + pad_rows, quarter), bf16),
            pltpu.VMEM((2 * rank + pad_rows, quarter), bf16),
            pltpu.VMEM((2 * rank + pad_rows, quarter), bf16),
            pltpu.VMEM((2 * rank + pad_rows, quarter), bf16),
            pltpu.VMEM((rank + pad_rows, quarter), bf16),
            pltpu.VMEM((rank + pad_rows, quarter), bf16),
            pltpu.VMEM((rank + pad_rows, quarter), bf16),
            pltpu.VMEM((rank + pad_rows, quarter), bf16),
            pltpu.VMEM((2, 4, rank + pad_rows, quarter), bf16),
            pltpu.VMEM((8, 128), f32),
            pltpu.VMEM((peers, 8, 128), f32),
            pltpu.SemaphoreType.REGULAR((5,)),
            dma(13),
            dma(9),
            dma(20 + 2 * chunks),
        ],
        compiler_params=pltpu.CompilerParams(
            collective_id=0, has_side_effects=True, vmem_limit_bytes=42 * MIB
        ),
        name="exchange",
    )(*held)

    pn, on, pcopy, ocopy, first, second, written = pl.pallas_call(
        write_kernel,
        in_specs=[vm] * 6,
        out_specs=[hbm] * 6 + [vm],
        out_shape=(
            shape(w_proj.shape, f32),
            shape(w_out.shape, f32),
            shape((d_model, width), bf16),
            shape((width, d_model), bf16),
            shape((2 * rank, width), f32),
            shape((2 * rank, width), f32),
            pltpu.VMEM((8, 128), f32),
        ),
        scratch_shapes=[dma(14)],
        compiler_params=pltpu.CompilerParams(vmem_limit_bytes=4 * MIB),
        name="write",
    )(pn, on, fp, fo, first, second)

    size = d_rows * (late_cuts[-1] - late_cuts[-2]) // pieces
    rest = d_rows - early * d_rows // chunks
    count = 2 * len(late_cuts) - 2
    lp, lo, fp, fo, up, uo = pl.pallas_call(
        relay_kernel,
        in_specs=[vm] * 6,
        out_specs=(vm,) * 6,
        out_shape=(
            pltpu.VMEM((rest, width), bf16),
            pltpu.VMEM((width, rest), bf16),
            pltpu.VMEM((rest - size, width), bf16),
            pltpu.VMEM((width, rest - size), bf16),
            pltpu.VMEM((size, width), f32),
            pltpu.VMEM((width, size), f32),
        ),
        scratch_shapes=[dma(2), dma(count)],
        compiler_params=pltpu.CompilerParams(
            collective_id=1, has_side_effects=True, vmem_limit_bytes=8 * MIB
        ),
        name="relay",
    )(written, held_f, d0, d1, gp, go)

    pcopy, ocopy = pl.pallas_call(
        finish_kernel,
        in_specs=[vm] * 6 + [hbm] * 2,
        out_specs=[hbm] * 2,
        out_shape=(shape(pcopy.shape, bf16), shape(ocopy.shape, bf16)),
        scratch_shapes=[pltpu.VMEM((size, width), bf16), pltpu.VMEM((width, size), bf16), dma(4)],
        input_output_aliases={6: 0, 7: 1},
        compiler_params=pltpu.CompilerParams(vmem_limit_bytes=4 * MIB),
        name="finish",
    )(lp, lo, fp, fo, up, uo, pcopy, ocopy)
    return pn, on, pcopy, ocopy, first.reshape(m1.shape), second.reshape(m2.shape)


def over_tokens(left_rows, right_rows, precise):
    return lax.dot_general(
        left_rows,
        right_rows,
        (((0,), (0,)), ((), ())),
        preferred_element_type=jnp.float32,
        precision=precise,
    )


def body(
    saved_inputs,
    proj_cotangent,
    saved_hidden,
    out_cotangent,
    factors,
    w_proj,
    w_out,
    moment_first,
    moment_second,
):
    highest = lax.Precision.HIGHEST
    fs_count = lax.axis_size("fs")
    tp_count = lax.axis_size("tp")
    d_model = factors.shape[1]
    hidden_width = proj_cotangent.shape[1]
    fs_rows = d_model // fs_count
    tp_feats = saved_inputs.shape[1]
    own_rows = lax.dynamic_slice_in_dim(factors, lax.axis_index("fs") * fs_rows, fs_rows, 1).astype(
        jnp.float32
    )
    own_feats = lax.dynamic_slice_in_dim(factors, lax.axis_index("tp") * tp_feats, tp_feats, 1)
    proj_rows = jnp.dot(saved_inputs, own_feats[0], preferred_element_type=jnp.float32)
    out_rows = jnp.dot(out_cotangent, own_feats[1], preferred_element_type=jnp.float32)
    proj_rows, out_rows = lax.psum((proj_rows, out_rows), "tp")
    partial_sums = jnp.stack(
        [
            over_tokens(proj_rows, proj_cotangent.astype(jnp.float32), highest),
            over_tokens(out_rows, saved_hidden.astype(jnp.float32), highest),
        ]
    )
    small_grads = lax.psum(partial_sums, "fs")
    first_next = beta_first * moment_first + (1.0 - beta_first) * small_grads
    second_next = beta_second * moment_second + (1.0 - beta_second) * small_grads * small_grads
    direction = first_next / (jnp.sqrt(second_next) + epsilon)
    update_full = jnp.einsum("kdr,kre->kde", own_rows, direction, precision=highest)
    squares = lax.psum(jnp.sum(update_full * update_full, axis=(1, 2)), ("fs", "tp"))
    norm_scale = lax.rsqrt(squares / (d_model * hidden_width * tp_count) + epsilon)
    stepped = update_full * norm_scale[:, None, None]
    proj_next = w_proj - learn_rate * stepped[0]
    out_next = w_out - learn_rate * stepped[1].T
    proj_copy, out_copy = (
        lax.all_gather(proj_next.astype(jnp.bfloat16), "fs", axis=0, tiled=True),
        lax.all_gather(out_next.astype(jnp.bfloat16), "fs", axis=1, tiled=True),
    )
    return (proj_next, out_next, proj_copy, out_copy, first_next, second_next)


def solution(mesh):
    placed = (
        P("fs", "tp"),
        P("fs", "tp"),
        P("fs", "tp"),
        P("fs", "tp"),
        P(),
        P("fs", "tp"),
        P("tp", "fs"),
        P(None, None, "tp"),
        P(None, None, "tp"),
    )
    planned = fast_body if mesh.shape["fs"] == 4 and mesh.shape["tp"] == 8 else body
    return jax.shard_map(
        planned,
        mesh=mesh,
        in_specs=placed,
        out_specs=(
            P("fs", "tp"),
            P("tp", "fs"),
            P(None, "tp"),
            P("tp", None),
            P(None, None, "tp"),
            P(None, None, "tp"),
        ),
        check_vma=False,
    )
```
